32 devices in a mesh: gr: 2 (over core), fs: 8 (over z, y), tp: 2 (over x).
Axes of the slice: x: 2, y: 2, z: 4, core: 2. Of those that a mesh axis runs over, the one named last changes fastest.
Arguments:
- tokens: bfloat16 [2048, 2048], P(('gr', 'fs')), may hold values from -60 to 60
- route_ids: int32 [2048, 2], P(('gr', 'fs')), may hold values from 0 to 7, all different within a row; in each aligned block of 128 rows (0 to 127, 128 to 255, ...) at most 32 rows name the same one
- route_logits: float32 [2048, 2], P(('gr', 'fs')), may hold values from -8 to 8
- norm_gain: float32 [2048], P(('gr', 'fs')), may hold values from 0.1 to 1.9
- gate_master: float32 [8, 2048, 7168], P(None, ('gr', 'fs'), 'tp'), may hold values from -0.125 to 0.125
- up_master: float32 [8, 2048, 7168], P(None, ('gr', 'fs'), 'tp'), may hold values from -0.125 to 0.125
- down_master: float32 [8, 7168, 2048], P(None, 'fs', ('gr', 'tp')), may hold values from -0.0625 to 0.0625
Outputs:
- gate_weight: bfloat16 [8, 2048, 7168], P('tp', None, 'fs')
- up_weight: bfloat16 [8, 2048, 7168], P('tp', None, 'fs')
- down_weight: bfloat16 [8, 7168, 2048], P('tp', 'fs')
- mixed: bfloat16 [2048, 2048], P(('gr', 'fs'))
The draws below stay inside these ranges and needn't reach their ends.
Inputs may be any that keep to these rules, and one draw needn't show every extreme that they name: `route_ids`: in the rows of one device, that is in each aligned block of 128 rows, each of the 8 experts is named by exactly 32 rows; a row names two different experts.
All inputs are finite; a program needn't handle non-finite values.
Results may differ from the reference program's by a relative error of at most 0.025.
Values may be sent and summed in bfloat16 or wider, within the bound.
A program may use at most 192 MiB of HBM per device.

```python
import math
import jax
import jax.numpy as jnp
import numpy as np
from jax import lax

D = 2048
FF = 7168
EXPERTS = 8
TOK_DEV = 128
CAP = 32
TOKENS = 2048
N_FS = 8
N_TP = 2


def draw_tokens(key, part):
    first_key = jax.random.fold_in(key, 11)
    second_key = jax.random.fold_in(key, 12)
    values = jnp.clip(jax.random.normal(first_key, (TOKENS, D), jnp.float32), -4.0, 4.0)
    scales = jnp.exp(jax.random.uniform(second_key, (TOKENS, 1), jnp.float32, 0.0, math.log(10.0)))
    return (values * scales).astype(jnp.bfloat16)


def level_of(own_key, shape, pieces, smallest, largest):
    loudness, own = 1.0, jax.random.fold_in(own_key, 6)
    for position, parts in pieces:
        heights = jnp.exp(jax.random.uniform(jax.random.fold_in(own, position), (parts,), jnp.float32, smallest / len(pieces), largest / len(pieces)))
        loudness = loudness * jnp.repeat(heights, shape[position] // parts).reshape([-1 if axis == position else 1 for axis in range(len(shape))])
    return loudness


def shared_out(rng, own, number, rows, count, top, reach, lean):
    order = jax.random.permutation(rng, count)
    crowded, usual = portions_of(count, rows * top, reach, lean, True), portions_of(count, rows * top, reach, lean, False)
    places = jnp.arange(count)

    def named(tallies, rotation):
        used = int((tallies > 0).sum())
        fixed = max(1, used // 4)
        passed = fixed + (places - fixed + rotation * (used - fixed)) % max(1, count - fixed)
        return jnp.zeros((count,), jnp.int32).at[order[jnp.where(places < fixed, places, passed)]].set(jnp.asarray(tallies, jnp.int32))

    tallies = jnp.where(number % 4 == 0, named(crowded, number // 4), named(usual, number - number // 4 - 1))
    mixed = jax.random.permutation(jax.random.fold_in(own, 3), count)
    giver, sink = mixed[0:count // 2 * 2:2], mixed[1:count // 2 * 2:2]
    margin = jnp.minimum(tallies[giver] - 1, reach - tallies[sink]) // 2
    margin = jnp.where((giver == order[0]) | (sink == order[0]) | (tallies[sink] == 0), 0, jnp.maximum(margin, 0))
    passed = jax.random.randint(jax.random.fold_in(own, 4), (count // 2,), 0, 1 << 20) % (margin + 1)
    tallies = tallies.at[giver].add(-passed).at[sink].add(passed)
    labels = jnp.searchsorted(jnp.cumsum(tallies), jnp.arange(rows * top), side="right").astype(jnp.int32)
    table = labels.reshape(top, rows).T
    table = table[jax.random.permutation(jax.random.fold_in(own, 1), rows)]
    rotation = jax.random.randint(jax.random.fold_in(own, 2), (rows, 1), 0, top)
    return jnp.take_along_axis(table, (jnp.arange(top)[None, :] + rotation) % top, axis=1)


def portions_of(number_of, total, reach, slope, full):
    portions = [(1 << 20) // math.isqrt(rank ** slope) + 1 for rank in range(1, number_of + 1)]
    largest = reach if full else min(reach, max(-(-total // number_of), total * portions[0] // sum(portions)))
    least = 1 if total - largest >= number_of - 1 else 0
    holding, rest = [largest] + [least] * (number_of - 1), total - largest - least * (number_of - 1)
    while rest > 0:
        movable = [i for i in range(1, number_of) if holding[i] < largest] or [i for i in range(1, number_of) if holding[i] < reach]
        whole, budget = sum([portions[i] for i in movable]), rest
        for i in movable:
            extra = min(reach - holding[i], max(1, budget * portions[i] // whole), rest)
            holding[i] = holding[i] + extra
            rest = rest - extra
    return np.array(holding)


def scatter_about(stream_key, dims, scale, limit, cuts=(), kind=jnp.bfloat16):
    loudness = level_of(stream_key, dims, cuts, -0.22, 0.18) if cuts else 1.0
    array = jax.random.normal(stream_key, dims, jnp.float32) * scale * loudness
    return jnp.minimum(jnp.maximum(array, -limit), limit).astype(kind)


def setup_inputs(seed: int = 0) -> dict:
    keys = jax.random.split(jax.random.key(seed), 8)
    tokens = draw_tokens(jax.random.fold_in(keys[7], 71), 0)
    route_ids_keys = jax.random.split(jax.random.fold_in(keys[1], 1), TOKENS // TOK_DEV)
    route_ids_turns = jax.random.permutation(jax.random.fold_in(keys[1], 3), TOKENS // TOK_DEV)
    route_ids = jax.vmap(lambda own, number: shared_out(jax.random.fold_in(keys[1], 2), own, number, TOK_DEV, EXPERTS, 2, CAP, 1))(route_ids_keys, route_ids_turns).reshape((TOKENS, 2))
    route_logits = scatter_about(keys[2], (TOKENS, 2), 1.5, 8.0, ((0, 16),), jnp.float32)
    norm_gain = jnp.clip(1.0 + 0.18 * jax.random.normal(keys[3], (D,), jnp.float32), 0.1, 1.9)
    gate_master = scatter_about(keys[4], (EXPERTS, D, FF), D ** -0.5, 0.125, ((1, 16), (2, 2)), jnp.float32)
    up_master = scatter_about(keys[5], (EXPERTS, D, FF), D ** -0.5, 0.125, ((1, 16), (2, 2)), jnp.float32)
    down_master = scatter_about(keys[6], (EXPERTS, FF, D), FF ** -0.5, 0.0625, ((1, 8), (2, 4)), jnp.float32)
    return {"tokens": tokens, "route_ids": route_ids, "route_logits": route_logits, "norm_gain": norm_gain, "gate_master": gate_master, "up_master": up_master, "down_master": down_master}


epsilon = 1e-06

def reference(tokens, route_ids, route_logits, norm_gain, gate_master, up_master, down_master):
    gate_weight = (gate_master * norm_gain[None, :, None]).astype(jnp.bfloat16)
    up_weight = (up_master * norm_gain[None, :, None]).astype(jnp.bfloat16)
    down_weight = down_master.astype(jnp.bfloat16)
    as_float = tokens.astype(jnp.float32)
    normed = (as_float * lax.rsqrt(lax.optimization_barrier(jnp.mean(as_float * as_float, axis=-1, keepdims=True)) + epsilon)).astype(jnp.bfloat16)
    differ = route_logits[:, 0] - route_logits[:, 1]
    route_weight = jnp.stack([jax.nn.sigmoid(differ), jax.nn.sigmoid(-differ)], axis=1)
    routed = TOKENS // 4
    positions = jnp.arange(TOKENS, dtype=jnp.int32)
    slice_width = FF // N_FS
    per_block = EXPERTS // N_TP

    def expert_part(expert):
        route_hits = route_ids == expert
        chosen = jnp.any(route_hits, axis=1)
        sort_key = jnp.where(chosen, positions, positions + TOKENS)
        order = jnp.argsort(sort_key)[:routed].astype(jnp.int32)
        weight_rows = lax.optimization_barrier(jnp.sum(jnp.where(route_hits, route_weight, 0.0), axis=1))[order]
        picked = normed[order]
        gate_act = jnp.dot(picked, gate_weight[expert], preferred_element_type=jnp.float32)
        up_act = jnp.dot(picked, up_weight[expert], preferred_element_type=jnp.float32)
        hidden = (jax.nn.silu(gate_act) * up_act).astype(jnp.bfloat16)
        down_expert = down_weight[expert]

        def add_slice(summed, slice_idx):
            begin = (slice_idx * slice_width).astype(jnp.int32)
            hidden_slice = lax.dynamic_slice_in_dim(hidden, begin, slice_width, 1)
            down_slice = lax.dynamic_slice_in_dim(down_expert, begin, slice_width, 0)
            partial_value = jnp.dot(hidden_slice, down_slice, preferred_element_type=jnp.float32)
            rounded = lax.optimization_barrier(partial_value.astype(jnp.bfloat16)).astype(jnp.float32)
            return (summed + rounded, None)
        expert_out, _ = lax.scan(add_slice, jnp.zeros((routed, D), jnp.float32), jnp.arange(N_FS, dtype=jnp.int32))
        return jnp.zeros((TOKENS, D), jnp.float32).at[order].add(expert_out * weight_rows[:, None])
    summed_all = jnp.zeros((TOKENS, D), jnp.float32)
    for tp_block in range(N_TP):
        block_sum = jnp.zeros((TOKENS, D), jnp.float32)
        for member in range(per_block):
            block_sum = block_sum + expert_part(tp_block * per_block + member)
        summed_all = summed_all + lax.optimization_barrier(block_sum.astype(jnp.bfloat16)).astype(jnp.float32)
    mixed = summed_all.astype(jnp.bfloat16)
    return (gate_weight, up_weight, down_weight, mixed)
```

```python
import functools

import jax
import jax.numpy as jnp
from jax import lax
from jax.experimental import pallas as pl
from jax.experimental.pallas import tpu as pltpu
from jax.sharding import PartitionSpec as P

CAP = 32


epsilon = 1e-06
MESH = pl.DeviceIdType.MESH
BF16 = jnp.bfloat16


def exchange_kernel(
    n_gr, n_fs, n_tp,
    gain_ref, gate_ref, up_ref, down_ref, packed_ref,
    gate_out, up_out, down_out, pieces,
    stage, stage_down, crossed, raw, raw_down,
    load_sem, load_down_sem, x_send, x_recv, s_send, s_recv, own_sem,
    d_send, d_recv, xd_send, xd_recv, own_down_sem, dd_send, dd_recv,
    p_send, p_recv, p_own,
):
    gr, fs, tp = (lax.axis_index(name) for name in ("gr", "fs", "tp"))
    experts, _, width = gate_out.shape
    rows, cols = gate_ref.shape[1], gate_ref.shape[2]
    per = cols // width
    down_cols = down_ref.shape[2]
    masters, outs = (gate_ref, up_ref), (gate_out, up_out)

    barrier = pltpu.get_barrier_semaphore()
    peers = 0
    for o in range(1, n_tp):
        pl.semaphore_signal(barrier, 1, device_id=(gr, fs, lax.rem(tp + o, n_tp)), device_id_type=MESH)
        peers += 1
    for k in range(1, n_fs):
        pl.semaphore_signal(barrier, 1, device_id=(gr, lax.rem(fs + k, n_fs), tp), device_id_type=MESH)
        peers += 1
    for o in range(1, n_gr):
        pl.semaphore_signal(barrier, 1, device_id=(lax.rem(gr + o, n_gr), fs, tp), device_id_type=MESH)
        peers += 1

    def tp_at(o):
        return lax.rem(tp + o, n_tp)

    order = [(w, o) for w in range(2) for o in [*range(1, n_tp), 0]]

    def load(e, w, o):
        return pltpu.make_async_copy(
            masters[w].at[tp_at(o) * experts + e], raw.at[w, o], load_sem.at[w, o]
        )

    def load_down(e, o):
        return pltpu.make_async_copy(
            down_ref.at[tp_at(o) * experts + e], raw_down.at[o], load_down_sem.at[o]
        )

    def over_tp(e, w, o, j):
        columns = pl.ds(j * width, width)
        return pltpu.make_async_remote_copy(
            stage.at[w, o, e, :, columns], crossed.at[w, o - 1, e, :, columns],
            x_send.at[w, o - 1, e, j], x_recv.at[w, o - 1, e, j],
            device_id=(gr, fs, tp_at(o)), device_id_type=MESH,
        )

    def rows_of(group, owner):
        return pl.ds(pl.multiple_of((group * n_fs + owner) * rows, rows), rows)

    def source(e, w, o, j):
        columns = pl.ds(j * width, width)
        if o == 0:
            return stage.at[w, 0, e, :, columns]
        return crossed.at[w, o - 1, e, :, columns]

    def fan(e, w, o):
        begin = lax.rem(tp - o + n_tp, n_tp) * per
        for j in range(per):
            if o:
                over_tp(e, w, o, j).wait_recv()
            to = begin + j
            k = lax.rem(to - fs + n_fs, n_fs)
            target = outs[w].at[e, rows_of(gr, fs)]

            @pl.when(to != fs)
            def _():
                pltpu.make_async_remote_copy(
                    source(e, w, o, j), target, s_send.at[w, e, k], s_recv.at[w, e, k],
                    device_id=(gr, to, tp), device_id_type=MESH,
                ).start()

            @pl.when(to == fs)
            def _():
                pltpu.make_async_copy(source(e, w, o, j), target, own_sem.at[w, e]).start()

    def arrival(e, w, k):
        piece = outs[w].at[e, rows_of(gr, lax.rem(fs - k + n_fs, n_fs))]
        return pltpu.make_async_remote_copy(
            piece, piece, s_send.at[w, e, k], s_recv.at[w, e, k],
            device_id=(gr, lax.rem(fs + k, n_fs), tp), device_id_type=MESH,
        )

    def own_copy(e, w):
        return pltpu.make_async_copy(
            source(e, w, 0, 0), outs[w].at[e, rows_of(gr, fs)], own_sem.at[w, e]
        )

    def over_gr(e, w, k, o, group):
        piece = outs[w].at[e, rows_of(group, lax.rem(fs - k + n_fs, n_fs))]
        return pltpu.make_async_remote_copy(
            piece, piece, d_send.at[w, e, k, o - 1], d_recv.at[w, e, k, o - 1],
            device_id=(lax.rem(gr + o, n_gr), fs, tp), device_id_type=MESH,
        )

    def down_block(group, t):
        return pl.ds(pl.multiple_of((group * n_tp + t) * down_cols, down_cols), down_cols)

    def down_over_tp(e, o):
        return pltpu.make_async_remote_copy(
            stage_down.at[o, e], down_out.at[e, :, down_block(gr, tp)],
            xd_send.at[o - 1, e], xd_recv.at[o - 1, e],
            device_id=(gr, fs, tp_at(o)), device_id_type=MESH,
        )

    def down_arrival(e, o):
        piece = down_out.at[e, :, down_block(gr, lax.rem(tp - o + n_tp, n_tp))]
        return pltpu.make_async_remote_copy(
            piece, piece, xd_send.at[o - 1, e], xd_recv.at[o - 1, e],
            device_id=(gr, fs, tp_at(o)), device_id_type=MESH,
        )

    def down_own(e):
        return pltpu.make_async_copy(
            stage_down.at[0, e], down_out.at[e, :, down_block(gr, tp)], own_down_sem.at[e]
        )

    def down_over_gr(e, s, o, group):
        piece = down_out.at[e, :, down_block(group, lax.rem(tp - s + n_tp, n_tp))]
        return pltpu.make_async_remote_copy(
            piece, piece, dd_send.at[e, s, o - 1], dd_recv.at[e, s, o - 1],
            device_id=(lax.rem(gr + o, n_gr), fs, tp), device_id_type=MESH,
        )

    pairs = n_fs // 2
    z, y = fs // 2, lax.rem(fs, 2)

    def relay(kind, hop):
        at = {"up": z - hop, "down": z + hop, "over": z - hop, "over_down": z + hop}[kind]
        to = {"up": fs + 2, "down": fs - 2}.get(kind, fs + 1 - 2 * y)
        origin = at * 2 + y
        here = packed_ref if hop == 0 else pieces.at[:, origin]
        slot = ["up", "down", "over", "over_down"].index(kind)
        return pltpu.make_async_remote_copy(
            here, pieces.at[:, origin], p_send.at[slot, hop], p_recv.at[origin],
            device_id=(gr, to, tp), device_id_type=MESH,
        )

    def landed(origin):
        piece = pieces.at[:, origin]
        return pltpu.make_async_remote_copy(
            piece, piece, p_send.at[0, 0], p_recv.at[origin],
            device_id=(gr, fs + 1 - 2 * y, tp), device_id_type=MESH,
        )

    def relayed(kind, hop):
        if kind == "up":
            return (z - hop >= 0) & (z + 1 < pairs)
        if kind == "down":
            return (z + hop < pairs) & (z >= 1)
        return z - hop >= 0 if kind == "over" else z + hop < pairs

    def relay_start(kind, hop):
        @pl.when(relayed(kind, hop))
        def _():
            relay(kind, hop).start()

    def relay_from(hop):
        @pl.when(z - hop >= 0)
        def _():
            landed((z - hop) * 2 + y).wait_recv()
            relay(kind="over", hop=hop).start()

        relay_start("up", hop)

        @pl.when(z + hop < pairs)
        def _():
            landed((z + hop) * 2 + y).wait_recv()
            relay(kind="over_down", hop=hop).start()

        relay_start("down", hop)

    own_piece = pltpu.make_async_copy(packed_ref, pieces.at[:, fs], p_own)

    for w, o in order:
        load(0, w, o).start()
    for o in range(n_tp):
        load_down(0, o).start()
    pl.semaphore_wait(barrier, peers)
    for kind in ("up", "down", "over"):
        relay_start(kind, 0)
    own_piece.start()

    def cast(e):
        for w, o in order:
            load(e, w, o).wait()
            stage[w, o, e] = (raw[w, o] * gain_ref[...]).astype(BF16)

            @pl.when(e + 1 < experts)
            def _():
                load(e + 1, w, o).start()

            if o:
                for j in range(per):
                    over_tp(e, w, o, j).start()
            else:
                fan(e, w, 0)

    def forward(e):
        for w in range(2):
            for o in range(1, n_tp):
                fan(e, w, o)

    cast(0)

    @pl.loop(1, experts)
    def _(e):
        cast(e)
        forward(e - 1)

    for hop in range(1, pairs):
        relay_from(hop)

    @pl.loop(0, experts)
    def _(e):
        for o in [*range(1, n_tp), 0]:
            load_down(e, o).wait()
            stage_down[o, e] = raw_down[o].astype(BF16)

            @pl.when(e + 1 < experts)
            def _():
                load_down(e + 1, o).start()

            if o:
                down_over_tp(e, o).start()
            else:
                down_own(e).start()

    def collect(e):
        for w in range(2):
            own_copy(e, w).wait()
            for o in range(1, n_gr):
                over_gr(e, w, 0, o, gr).start()

        @pl.loop(1, n_fs)
        def _(k):
            for w in range(2):
                arrival(e, w, k).wait_recv()
                for o in range(1, n_gr):
                    over_gr(e, w, k, o, gr).start()

    forward(experts - 1)

    @pl.loop(0, experts - 1)
    def _(e):
        collect(e)

    @pl.loop(0, experts)
    def _(e):
        down_own(e).wait()
        for s in range(1, n_tp):
            down_arrival(e, s).wait_recv()
        for s in range(n_tp):
            for o in range(1, n_gr):
                down_over_gr(e, s, o, gr).start()

    collect(experts - 1)

    @pl.loop(0, experts)
    def _(e):
        for w in range(2):
            for o in range(1, n_tp):
                for j in range(per):
                    over_tp(e, w, o, j).wait_send()

            @pl.loop(1, n_fs)
            def _(k):
                arrival(e, w, k).wait_send()

            @pl.loop(0, n_fs)
            def _(k):
                for o in range(1, n_gr):
                    over_gr(e, w, k, o, gr).wait_send()
                    over_gr(e, w, k, o, lax.rem(gr - o + n_gr, n_gr)).wait_recv()

        for s in range(1, n_tp):
            down_over_tp(e, s).wait_send()
        for s in range(n_tp):
            for o in range(1, n_gr):
                down_over_gr(e, s, o, gr).wait_send()
                down_over_gr(e, s, o, lax.rem(gr - o + n_gr, n_gr)).wait_recv()

    own_piece.wait()
    for at in range(pairs):
        landed(at * 2 + 1 - y).wait_recv()
    for kind in ("up", "down", "over", "over_down"):
        for hop in range(1 if kind == "over_down" else 0, pairs):
            @pl.when(relayed(kind, hop))
            def _():
                relay(kind, hop).wait_send()


def exchange(sizes, norm_gain, gate_master, up_master, down_master, packed):
    n_gr, n_fs, n_tp = sizes
    all_experts, rows, cols = gate_master.shape
    experts = all_experts // n_tp
    width = cols * n_tp // n_fs
    hidden, down_cols = down_master.shape[1], down_master.shape[2]
    any_spec = pl.BlockSpec(memory_space=pl.ANY)
    dma = pltpu.SemaphoreType.DMA
    up_shape = jax.ShapeDtypeStruct((experts, rows * n_gr * n_fs, width), BF16)
    return pl.pallas_call(
        functools.partial(exchange_kernel, n_gr, n_fs, n_tp),
        out_shape=(
            up_shape,
            up_shape,
            jax.ShapeDtypeStruct((experts, hidden, down_cols * n_gr * n_tp), BF16),
            jax.ShapeDtypeStruct((packed.shape[0], n_fs, *packed.shape[1:]), BF16),
        ),
        in_specs=[pl.BlockSpec(memory_space=pltpu.VMEM), *[any_spec] * 4],
        out_specs=(any_spec,) * 4,
        scratch_shapes=[
            pltpu.VMEM((2, n_tp, experts, rows, cols), BF16),
            pltpu.VMEM((n_tp, experts, hidden, down_cols), BF16),
            pltpu.VMEM((2, n_tp - 1, experts, rows, cols), BF16),
            pltpu.VMEM((2, n_tp, rows, cols), jnp.float32),
            pltpu.VMEM((n_tp, hidden, down_cols), jnp.float32),
            dma((2, n_tp)),
            dma((n_tp,)),
            dma((2, n_tp - 1, experts, n_fs // n_tp)),
            dma((2, n_tp - 1, experts, n_fs // n_tp)),
            dma((2, experts, n_fs)),
            dma((2, experts, n_fs)),
            dma((2, experts)),
            dma((2, experts, n_fs, n_gr - 1)),
            dma((2, experts, n_fs, n_gr - 1)),
            dma((n_tp - 1, experts)),
            dma((n_tp - 1, experts)),
            dma((experts,)),
            dma((experts, n_tp, n_gr - 1)),
            dma((experts, n_tp, n_gr - 1)),
            dma((4, n_fs // 2)),
            dma((n_fs,)),
            dma,
        ],
        compiler_params=pltpu.CompilerParams(
            collective_id=0, has_side_effects=True, vmem_limit_bytes=52 * 1024 * 1024
        ),
        cost_estimate=pl.CostEstimate(flops=0, bytes_accessed=1_000_000_000, transcendentals=0),
    )(norm_gain[:, None], gate_master, up_master, down_master, packed)


def experts_kernel(
    slices, lead,
    pieces, gate_in, up_in, down_in,
    gate_out, up_out, down_out, sums,
    tall, wide, partial, gate_act, up_act, hidden,
    tall_load, tall_store, wide_load, wide_store,
):
    experts, features, width = gate_in.shape
    depth, cols = tall.shape[1], wide.shape[2]
    steps, ring = 2 * slices, tall.shape[0]
    count = hidden.shape[1]
    owners, tokens = sums.shape[0], sums.shape[1]
    ins, outs = (gate_in, up_in), (gate_out, up_out)

    def tall_ends(refs, e, j):
        return refs[j % 2].at[e, pl.ds(j // 2 * depth, depth)]

    def tall_slot(e, j):
        return lax.rem(e * steps + j, ring)

    def load_tall(e, j):
        slot = tall_slot(e, j)
        return pltpu.make_async_copy(tall_ends(ins, e, j), tall.at[slot], tall_load.at[slot])

    def store_tall(e, j):
        slot = tall_slot(e, j)
        return pltpu.make_async_copy(tall.at[slot], tall_ends(outs, e, j), tall_store.at[slot])

    def span(c):
        return pl.ds(pl.multiple_of(c * cols, cols), cols)

    def load_wide(c, e):
        slot = c * experts + e
        return pltpu.make_async_copy(down_in.at[e, :, span(c)], wide.at[slot], wide_load.at[slot])

    def store_wide(c, e):
        slot = c * experts + e
        return pltpu.make_async_copy(wide.at[slot], down_out.at[e, :, span(c)], wide_store.at[slot])

    for j in range(lead):
        load_tall(j // steps, j % steps).start()

    @pl.loop(0, experts)
    def _(e):
        for j in range(steps):
            load_tall(e, j).wait()
            store_tall(e, j).start()
            later, k = e + (j + lead) // steps, (j + lead) % steps

            @pl.when(later < experts)
            def _():
                @pl.when(later * steps + k >= ring)
                def _():
                    before = later * steps + k - ring
                    store_tall(before // steps, k).wait()

                load_tall(later, k).start()

            @pl.when(e == experts - 1)
            def _():
                for i in range(j, slices * experts // 2, steps):
                    load_wide(i // experts, i % experts).start()

            act = (gate_act, up_act)[j % 2]
            x = pieces[e, :, :, pl.ds(j // 2 * depth, depth)].reshape(count, depth)
            value = jnp.dot(x, tall[tall_slot(e, j)], preferred_element_type=jnp.float32)
            if j < 2:
                act[...] = value
            else:
                act[...] += value
        hidden[e] = (jax.nn.silu(gate_act[...]) * up_act[...]).astype(BF16)

    half = slices * experts // 2

    @pl.loop(0, slices)
    def _(c):
        for e in range(experts):
            load_wide(c, e).wait()
            store_wide(c, e).start()
            ahead = c * experts + e + half

            @pl.when(ahead < slices * experts)
            def _():
                load_wide(ahead // experts, lax.rem(ahead, experts)).start()

            value = jnp.dot(hidden[e], wide[c * experts + e], preferred_element_type=jnp.float32)
            partial[e] = value.astype(BF16).reshape(partial.shape[1:])

        for o in range(owners):
            weights = pieces[:, o, :, pl.ds(features, tokens)].reshape(-1, tokens)
            rows = partial[:, o].reshape(-1, cols)
            sums[o, :, span(c)] = lax.dot_general(
                weights, rows, (((0,), (0,)), ((), ())), preferred_element_type=jnp.float32
            ).astype(BF16)

    for i in range(ring):
        at = experts * steps - ring + i
        store_tall(at // steps, at % steps).wait()
    for c in range(slices):
        for e in range(experts):
            store_wide(c, e).wait()


def run_experts(pieces, gate, up, down):
    experts, features, width = gate.shape
    _, owners, cap, padded = pieces.shape
    tokens, count, slices = padded - features, owners * cap, 4
    ring = 2 * 2 * slices
    any_spec = pl.BlockSpec(memory_space=pl.ANY)
    vmem = pl.BlockSpec(memory_space=pltpu.VMEM)
    dma = pltpu.SemaphoreType.DMA
    return pl.pallas_call(
        functools.partial(experts_kernel, slices, 2 * slices),
        out_shape=(
            jax.ShapeDtypeStruct(gate.shape, BF16),
            jax.ShapeDtypeStruct(up.shape, BF16),
            jax.ShapeDtypeStruct(down.shape, BF16),
            jax.ShapeDtypeStruct((owners, tokens, features), BF16),
        ),
        in_specs=[vmem, any_spec, any_spec, any_spec],
        out_specs=(any_spec, any_spec, any_spec, vmem),
        scratch_shapes=[
            pltpu.VMEM((ring, features // slices, width), BF16),
            pltpu.VMEM((slices * experts, width, features // slices), BF16),
            pltpu.VMEM((experts, owners, cap, features // slices), BF16),
            pltpu.VMEM((count, width), jnp.float32),
            pltpu.VMEM((count, width), jnp.float32),
            pltpu.VMEM((experts, count, width), BF16),
            dma((ring,)),
            dma((ring,)),
            dma((slices * experts,)),
            dma((slices * experts,)),
        ],
        compiler_params=pltpu.CompilerParams(vmem_limit_bytes=44 * 1024 * 1024),
        cost_estimate=pl.CostEstimate(
            flops=6 * experts * count * features * width,
            bytes_accessed=12 * experts * features * width, transcendentals=0,
        ),
    )(pieces, gate, up, down)


def plan_of(n_bits, features):
    rest = list(range(2, n_bits))
    orders = ([0, "x", 1, *rest], ["x", 1, 0, *rest], [1, 0, "x", *rest])
    unit = 128
    units = features // unit
    shares, chunks, begin = [], [], 0
    for i in range(6):
        shares.append((units - sum(shares)) // (6 - i))
    for i, share in enumerate(shares):
        if share:
            chunks.append((orders[i % 3], begin * unit, share * unit))
        begin += share
    return chunks


def combine_kernel(n_fs, chunks, sums, out, acc, *rest):
    stages = len(chunks[0][0])
    boxes, (s_send, s_recv, o_send, o_recv) = rest[:-4], rest[-4:]
    gr, fs, tp = (lax.axis_index(name) for name in ("gr", "fs", "tp"))
    n_bits = stages - 1
    rows = sums.shape[-2]
    bits = [lax.rem(fs // (1 << b), 2) for b in range(n_bits)]

    def mine(dim):
        return tp if dim == "x" else bits[dim]

    def partner(dim):
        if dim == "x":
            return (gr, fs, 1 - tp)
        return (gr, fs + (1 - 2 * bits[dim]) * (1 << dim), tp)

    def block(order, stage, own, cols):
        index = [slice(None)] * (n_bits + 1)
        for dim in order[: stage + 1]:
            at = n_bits if dim == "x" else n_bits - 1 - dim
            index[at] = mine(dim)
            if dim == order[stage] and not own:
                index[at] = 1 - mine(dim)
        return (*index, slice(None), cols)

    barrier = pltpu.get_barrier_semaphore()
    for dim in [*range(n_bits), "x"]:
        pl.semaphore_signal(barrier, 1, device_id=partner(dim), device_id_type=MESH)
    pl.semaphore_wait(barrier, n_bits + 1)

    def step(i, stage):
        order, begin, size = chunks[i]
        held = sums if stage == 0 else acc
        return pltpu.make_async_remote_copy(
            held.at[block(order, stage, False, pl.ds(begin, size))],
            boxes[i * stages + stage], s_send.at[i, stage], s_recv.at[i, stage],
            device_id=partner(order[stage]), device_id_type=MESH,
        )

    def finished(i):
        _, begin, size = chunks[i]
        here = out.at[pl.ds(pl.multiple_of(tp * rows, rows), rows), pl.ds(begin, size)]
        return pltpu.make_async_remote_copy(
            here, here, o_send.at[i], o_recv.at[i], device_id=partner("x"), device_id_type=MESH
        )

    for i in range(len(chunks)):
        step(i, 0).start()
    for stage in range(stages):
        for i, (order, begin, size) in enumerate(chunks):
            step(i, stage).wait_recv()
            at = block(order, stage, True, pl.ds(begin, size))
            held = sums if stage == 0 else acc
            value = held[at].astype(jnp.float32) + boxes[i * stages + stage][...].astype(jnp.float32)
            if stage + 1 < stages:
                acc[at] = value.astype(BF16)
                step(i, stage + 1).start()
            else:
                out[pl.ds(pl.multiple_of(tp * rows, rows), rows), pl.ds(begin, size)] = value.astype(BF16)
                finished(i).start()
    for i in range(len(chunks)):
        _, begin, size = chunks[i]
        there = out.at[pl.ds(pl.multiple_of((1 - tp) * rows, rows), rows), pl.ds(begin, size)]
        pltpu.make_async_remote_copy(
            there, there, o_send.at[i], o_recv.at[i], device_id=partner("x"), device_id_type=MESH
        ).wait_recv()
        finished(i).wait_send()
        for stage in range(stages):
            step(i, stage).wait_send()


def combine(n_fs, sums):
    owners, tokens, features = sums.shape
    n_bits = n_fs.bit_length() - 1
    stages, rows = n_bits + 1, tokens // 2
    chunks = plan_of(n_bits, features)
    dma = pltpu.SemaphoreType.DMA
    vmem = pl.BlockSpec(memory_space=pltpu.VMEM)
    boxes = [
        pltpu.VMEM((*(2,) * (n_bits - stage), rows, size), BF16)
        for _, _, size in chunks for stage in range(stages)
    ]
    view = (*(2,) * (n_bits + 1), rows, features)
    return pl.pallas_call(
        functools.partial(combine_kernel, n_fs, chunks),
        out_shape=jax.ShapeDtypeStruct((tokens, features), BF16),
        in_specs=[vmem],
        out_specs=vmem,
        scratch_shapes=[
            pltpu.VMEM(view, BF16),
            *boxes,
            dma((len(chunks), stages)),
            dma((len(chunks), stages)),
            dma((len(chunks),)),
            dma((len(chunks),)),
        ],
        compiler_params=pltpu.CompilerParams(
            collective_id=1, has_side_effects=True, vmem_limit_bytes=40 * 1024 * 1024
        ),
    )(sums.reshape(view))


def plain_local(tokens, route_ids, route_logits, norm_gain, gate_master, up_master, down_master):
    gain_rows = norm_gain[None, :, None]
    gate_half = (gate_master * gain_rows).astype(jnp.bfloat16)
    up_half = (up_master * gain_rows).astype(jnp.bfloat16)
    down_half = down_master.astype(jnp.bfloat16)
    gate_cols, up_cols, down_cols = (
        lax.all_to_all(gate_half, "tp", split_axis=0, concat_axis=2, tiled=True),
        lax.all_to_all(up_half, "tp", split_axis=0, concat_axis=2, tiled=True),
        lax.all_to_all(down_half, "tp", split_axis=0, concat_axis=2, tiled=True),
    )
    gate_part, up_part = (
        lax.all_to_all(gate_cols, "fs", split_axis=2, concat_axis=1, tiled=True),
        lax.all_to_all(up_cols, "fs", split_axis=2, concat_axis=1, tiled=True),
    )
    gate_weight, up_weight, down_weight = (
        lax.all_gather(gate_part, "gr", axis=1, tiled=True),
        lax.all_gather(up_part, "gr", axis=1, tiled=True),
        lax.all_gather(down_cols, "gr", axis=2, tiled=True),
    )
    as_float = tokens.astype(jnp.float32)
    normed = (
        as_float * lax.rsqrt(jnp.mean(as_float * as_float, axis=-1, keepdims=True) + epsilon)
    ).astype(jnp.bfloat16)
    differ = route_logits[:, 0] - route_logits[:, 1]
    route_weight = jnp.stack([jax.nn.sigmoid(differ), jax.nn.sigmoid(-differ)], axis=1)
    experts_here = gate_weight.shape[0]
    first_expert = lax.axis_index("tp") * experts_here
    expert_ids = first_expert + jnp.arange(experts_here, dtype=jnp.int32)
    route_hits = route_ids[None, :, :] == expert_ids[:, None, None]
    chosen = jnp.any(route_hits, axis=2)
    weight_rows = jnp.sum(jnp.where(route_hits, route_weight[None, :, :], 0.0), axis=2)
    slot_rank = jnp.cumsum(chosen.astype(jnp.int32), axis=1) - 1
    slot_ids = jnp.arange(CAP, dtype=jnp.int32)
    picker = chosen[:, None, :] & (slot_rank[:, None, :] == slot_ids[None, :, None])
    picker_float = picker.astype(jnp.float32)
    packed = jnp.einsum(
        "xsr,rd->sxd", picker.astype(jnp.bfloat16), normed, preferred_element_type=jnp.float32
    ).astype(jnp.bfloat16)
    slot_weight = jnp.einsum(
        "xsr,xr->sx", picker_float, weight_rows, precision=lax.Precision.HIGHEST
    )
    pieces = lax.all_gather(packed, "fs", axis=0, tiled=True)
    gate_act = jnp.einsum("kxd,xdh->kxh", pieces, gate_weight, preferred_element_type=jnp.float32)
    up_act = jnp.einsum("kxd,xdh->kxh", pieces, up_weight, preferred_element_type=jnp.float32)
    hidden = (jax.nn.silu(gate_act) * up_act).astype(jnp.bfloat16)
    expert_out = lax.psum_scatter(
        jnp.einsum("kxh,xhd->kxd", hidden, down_weight, preferred_element_type=jnp.float32).astype(
            jnp.bfloat16
        ),
        "fs",
        scatter_dimension=0,
        tiled=True,
    ).astype(jnp.float32)
    weighted = expert_out * slot_weight[:, :, None]
    block_sum = jnp.einsum("xsr,sxd->rd", picker_float, weighted, precision=lax.Precision.HIGHEST)
    mixed = lax.psum(block_sum.astype(jnp.bfloat16), "tp")
    return (gate_weight, up_weight, down_weight, mixed)


def fast_local(sizes, tokens, route_ids, route_logits, norm_gain, gate_master, up_master, down_master):
    n_gr, n_fs, n_tp = sizes
    as_float = tokens.astype(jnp.float32)
    normed = (
        as_float * lax.rsqrt(jnp.mean(as_float * as_float, axis=-1, keepdims=True) + epsilon)
    ).astype(jnp.bfloat16)
    differ = route_logits[:, 0] - route_logits[:, 1]
    route_weight = jnp.stack([jax.nn.sigmoid(differ), jax.nn.sigmoid(-differ)], axis=1)
    experts_here = gate_master.shape[0] // n_tp
    first_expert = lax.axis_index("tp") * experts_here
    expert_ids = first_expert + jnp.arange(experts_here, dtype=jnp.int32)
    route_hits = route_ids[None, :, :] == expert_ids[:, None, None]
    chosen = jnp.any(route_hits, axis=2)
    weight_rows = jnp.sum(jnp.where(route_hits, route_weight[None, :, :], 0.0), axis=2)
    slot_rank = jnp.cumsum(chosen.astype(jnp.int32), axis=1) - 1
    slot_ids = jnp.arange(CAP, dtype=jnp.int32)
    picker = chosen[:, None, :] & (slot_rank[:, None, :] == slot_ids[None, :, None])
    packed = jnp.einsum(
        "xsr,rd->xsd", picker.astype(jnp.bfloat16), normed, preferred_element_type=jnp.float32
    ).astype(jnp.bfloat16)
    combiner = (picker.astype(jnp.float32) * weight_rows[:, None, :]).astype(jnp.bfloat16)
    gate_moved, up_moved, down_moved, pieces = exchange(
        sizes, norm_gain, gate_master, up_master, down_master,
        jnp.concatenate([packed, combiner], axis=2),
    )
    gate_weight, up_weight, down_weight, sums = run_experts(
        pieces, gate_moved, up_moved, down_moved
    )
    return (gate_weight, up_weight, down_weight, combine(n_fs, sums))


def solution(mesh):
    n_gr, n_fs, n_tp = (mesh.shape[name] for name in ("gr", "fs", "tp"))
    placed = (
        P(("gr", "fs"), None),
        P(("gr", "fs"), None),
        P(("gr", "fs"), None),
        P(("gr", "fs")),
        P(None, ("gr", "fs"), "tp"),
        P(None, ("gr", "fs"), "tp"),
        P(None, "fs", ("gr", "tp")),
    )

    def local(tokens, route_ids, route_logits, norm_gain, gate_master, up_master, down_master):
        width = gate_master.shape[2] * n_tp // n_fs
        aligned = width % 128 == 0 and down_master.shape[2] % 128 == 0
        fits = n_fs % n_tp == 0 and n_fs & (n_fs - 1) == 0 and n_fs > 2
        fits = fits and n_gr > 1 and n_tp == 2 and tokens.shape[0] % 128 == 0
        run = functools.partial(fast_local, (n_gr, n_fs, n_tp)) if aligned and fits else plain_local
        return run(tokens, route_ids, route_logits, norm_gain, gate_master, up_master, down_master)

    return jax.shard_map(
        local,
        mesh=mesh,
        in_specs=placed,
        out_specs=(
            P("tp", None, "fs"),
            P("tp", None, "fs"),
            P("tp", "fs", None),
            P(("gr", "fs"), None),
        ),
        check_vma=False,
    )
```

```python
import functools

import jax
import jax.numpy as jnp
from jax import lax
from jax.experimental import pallas as pl
from jax.experimental.pallas import tpu as pltpu
from jax.sharding import PartitionSpec as P

CAP = 32


epsilon = 1e-06
MESH = pl.DeviceIdType.MESH
BF16 = jnp.bfloat16


def exchange_kernel(
    n_gr, n_fs, n_tp,
    gain_ref, gate_ref, up_ref, down_ref, packed_ref,
    gate_out, up_out, down_out, pieces,
    stage, stage_down, crossed, raw, raw_down,
    load_sem, load_down_sem, x_send, x_recv, s_send, s_recv, own_sem,
    d_send, d_recv, xd_send, xd_recv, own_down_sem, dd_send, dd_recv,
    p_send, p_recv, p_own,
):
    gr, fs, tp = (lax.axis_index(name) for name in ("gr", "fs", "tp"))
    experts, _, width = gate_out.shape
    rows, cols = gate_ref.shape[1], gate_ref.shape[2]
    per = cols // width
    down_cols = down_ref.shape[2]
    masters, outs = (gate_ref, up_ref), (gate_out, up_out)

    barrier = pltpu.get_barrier_semaphore()
    peers = 0
    for o in range(1, n_tp):
        pl.semaphore_signal(barrier, 1, device_id=(gr, fs, lax.rem(tp + o, n_tp)), device_id_type=MESH)
        peers += 1
    for k in range(1, n_fs):
        pl.semaphore_signal(barrier, 1, device_id=(gr, lax.rem(fs + k, n_fs), tp), device_id_type=MESH)
        peers += 1
    for o in range(1, n_gr):
        pl.semaphore_signal(barrier, 1, device_id=(lax.rem(gr + o, n_gr), fs, tp), device_id_type=MESH)
        peers += 1

    def tp_at(o):
        return lax.rem(tp + o, n_tp)

    order = [(w, o) for w in range(2) for o in [*range(1, n_tp), 0]]

    def load(e, w, o):
        return pltpu.make_async_copy(
            masters[w].at[tp_at(o) * experts + e], raw.at[w, o], load_sem.at[w, o]
        )

    def load_down(e, o):
        return pltpu.make_async_copy(
            down_ref.at[tp_at(o) * experts + e], raw_down.at[o], load_down_sem.at[o]
        )

    def over_tp(e, w, o, j):
        columns = pl.ds(j * width, width)
        return pltpu.make_async_remote_copy(
            stage.at[w, o, e, :, columns], crossed.at[w, o - 1, e, :, columns],
            x_send.at[w, o - 1, e, j], x_recv.at[w, o - 1, e, j],
            device_id=(gr, fs, tp_at(o)), device_id_type=MESH,
        )

    def rows_of(group, owner):
        return pl.ds(pl.multiple_of((group * n_fs + owner) * rows, rows), rows)

    def source(e, w, o, j):
        columns = pl.ds(j * width, width)
        if o == 0:
            return stage.at[w, 0, e, :, columns]
        return crossed.at[w, o - 1, e, :, columns]

    def fan(e, w, o):
        begin = lax.rem(tp - o + n_tp, n_tp) * per
        for j in range(per):
            if o:
                over_tp(e, w, o, j).wait_recv()
            to = begin + j
            k = lax.rem(to - fs + n_fs, n_fs)
            target = outs[w].at[e, rows_of(gr, fs)]

            @pl.when(to != fs)
            def _():
                pltpu.make_async_remote_copy(
                    source(e, w, o, j), target, s_send.at[w, e, k], s_recv.at[w, e, k],
                    device_id=(gr, to, tp), device_id_type=MESH,
                ).start()

            @pl.when(to == fs)
            def _():
                pltpu.make_async_copy(source(e, w, o, j), target, own_sem.at[w, e]).start()

    def arrival(e, w, k):
        piece = outs[w].at[e, rows_of(gr, lax.rem(fs - k + n_fs, n_fs))]
        return pltpu.make_async_remote_copy(
            piece, piece, s_send.at[w, e, k], s_recv.at[w, e, k],
            device_id=(gr, lax.rem(fs + k, n_fs), tp), device_id_type=MESH,
        )

    def own_copy(e, w):
        return pltpu.make_async_copy(
            source(e, w, 0, 0), outs[w].at[e, rows_of(gr, fs)], own_sem.at[w, e]
        )

    def over_gr(e, w, k, o, group):
        piece = outs[w].at[e, rows_of(group, lax.rem(fs - k + n_fs, n_fs))]
        return pltpu.make_async_remote_copy(
            piece, piece, d_send.at[w, e, k, o - 1], d_recv.at[w, e, k, o - 1],
            device_id=(lax.rem(gr + o, n_gr), fs, tp), device_id_type=MESH,
        )

    def down_block(group, t):
        return pl.ds(pl.multiple_of((group * n_tp + t) * down_cols, down_cols), down_cols)

    def down_over_tp(e, o):
        return pltpu.make_async_remote_copy(
            stage_down.at[o, e], down_out.at[e, :, down_block(gr, tp)],
            xd_send.at[o - 1, e], xd_recv.at[o - 1, e],
            device_id=(gr, fs, tp_at(o)), device_id_type=MESH,
        )

    def down_arrival(e, o):
        piece = down_out.at[e, :, down_block(gr, lax.rem(tp - o + n_tp, n_tp))]
        return pltpu.make_async_remote_copy(
            piece, piece, xd_send.at[o - 1, e], xd_recv.at[o - 1, e],
            device_id=(gr, fs, tp_at(o)), device_id_type=MESH,
        )

    def down_own(e):
        return pltpu.make_async_copy(
            stage_down.at[0, e], down_out.at[e, :, down_block(gr, tp)], own_down_sem.at[e]
        )

    def down_over_gr(e, s, o, group):
        piece = down_out.at[e, :, down_block(group, lax.rem(tp - s + n_tp, n_tp))]
        return pltpu.make_async_remote_copy(
            piece, piece, dd_send.at[e, s, o - 1], dd_recv.at[e, s, o - 1],
            device_id=(lax.rem(gr + o, n_gr), fs, tp), device_id_type=MESH,
        )

    pairs = n_fs // 2
    z, y = fs // 2, lax.rem(fs, 2)

    def relay(kind, hop, e):
        at = {"up": z - hop, "down": z + hop, "over": z - hop, "over_down": z + hop}[kind]
        to = {"up": fs + 2, "down": fs - 2}.get(kind, fs + 1 - 2 * y)
        origin = at * 2 + y
        here = packed_ref.at[e] if hop == 0 else pieces.at[e, origin]
        slot = ["up", "down", "over", "over_down"].index(kind)
        return pltpu.make_async_remote_copy(
            here, pieces.at[e, origin], p_send.at[slot, hop, e], p_recv.at[origin, e],
            device_id=(gr, to, tp), device_id_type=MESH,
        )

    def landed(origin, e):
        piece = pieces.at[e, origin]
        return pltpu.make_async_remote_copy(
            piece, piece, p_send.at[0, 0, e], p_recv.at[origin, e],
            device_id=(gr, fs + 1 - 2 * y, tp), device_id_type=MESH,
        )

    def relayed(kind, hop):
        if kind == "up":
            return (z - hop >= 0) & (z + 1 < pairs)
        if kind == "down":
            return (z + hop < pairs) & (z >= 1)
        return z - hop >= 0 if kind == "over" else z + hop < pairs

    def relay_start(kind, hop, e):
        @pl.when(relayed(kind, hop))
        def _():
            relay(kind, hop, e).start()

    def relay_from(hop):
        for e in range(experts):
            @pl.when(z - hop >= 0)
            def _():
                landed((z - hop) * 2 + y, e).wait_recv()

            relay_start("up", hop, e)
            relay_start("over", hop, e)

            @pl.when(z + hop < pairs)
            def _():
                landed((z + hop) * 2 + y, e).wait_recv()

            relay_start("down", hop, e)
            relay_start("over_down", hop, e)

    own_piece = pltpu.make_async_copy(packed_ref, pieces.at[:, fs], p_own)

    for w, o in order:
        load(0, w, o).start()
    for o in range(n_tp):
        load_down(0, o).start()
    pl.semaphore_wait(barrier, peers)
    for kind in ("up", "down", "over"):
        for e in range(experts):
            relay_start(kind, 0, e)
    own_piece.start()

    def cast(e, leg):
        for w, o in order:
            if (o > 0) != (leg == "tp"):
                continue
            load(e, w, o).wait()
            stage[w, o, e] = (raw[w, o] * gain_ref[...]).astype(BF16)

            @pl.when(e + 1 < experts)
            def _():
                load(e + 1, w, o).start()

            if o:
                for j in range(per):
                    over_tp(e, w, o, j).start()
            else:
                fan(e, w, 0)

    def forward(e):
        for w in range(2):
            for o in range(1, n_tp):
                fan(e, w, o)

    cast(0, "tp")
    for hop in range(1, pairs):
        relay_from(hop)
    cast(0, "fs")

    @pl.loop(1, experts)
    def _(e):
        cast(e, "tp")
        cast(e, "fs")
        forward(e - 1)

    @pl.loop(0, experts)
    def _(e):
        for o in [*range(1, n_tp), 0]:
            load_down(e, o).wait()
            stage_down[o, e] = raw_down[o].astype(BF16)

            @pl.when(e + 1 < experts)
            def _():
                load_down(e + 1, o).start()

            if o:
                down_over_tp(e, o).start()
            else:
                down_own(e).start()

    def collect(e):
        for w in range(2):
            own_copy(e, w).wait()
            for o in range(1, n_gr):
                over_gr(e, w, 0, o, gr).start()

        @pl.loop(1, n_fs)
        def _(k):
            for w in range(2):
                arrival(e, w, k).wait_recv()
                for o in range(1, n_gr):
                    over_gr(e, w, k, o, gr).start()

    forward(experts - 1)

    @pl.loop(0, experts - 1)
    def _(e):
        collect(e)

    @pl.loop(0, experts)
    def _(e):
        down_own(e).wait()
        for s in range(1, n_tp):
            down_arrival(e, s).wait_recv()
        for s in range(n_tp):
            for o in range(1, n_gr):
                down_over_gr(e, s, o, gr).start()

    collect(experts - 1)

    @pl.loop(0, experts)
    def _(e):
        for w in range(2):
            for o in range(1, n_tp):
                for j in range(per):
                    over_tp(e, w, o, j).wait_send()

            @pl.loop(1, n_fs)
            def _(k):
                arrival(e, w, k).wait_send()

            @pl.loop(0, n_fs)
            def _(k):
                for o in range(1, n_gr):
                    over_gr(e, w, k, o, gr).wait_send()
                    over_gr(e, w, k, o, lax.rem(gr - o + n_gr, n_gr)).wait_recv()

        for s in range(1, n_tp):
            down_over_tp(e, s).wait_send()
        for s in range(n_tp):
            for o in range(1, n_gr):
                down_over_gr(e, s, o, gr).wait_send()
                down_over_gr(e, s, o, lax.rem(gr - o + n_gr, n_gr)).wait_recv()

    own_piece.wait()
    for at in range(pairs):
        for e in range(experts):
            landed(at * 2 + 1 - y, e).wait_recv()
    for kind in ("up", "down", "over", "over_down"):
        for hop in range(1 if kind == "over_down" else 0, pairs):
            @pl.when(relayed(kind, hop))
            def _():
                for e in range(experts):
                    relay(kind, hop, e).wait_send()


def exchange(sizes, norm_gain, gate_master, up_master, down_master, packed):
    n_gr, n_fs, n_tp = sizes
    all_experts, rows, cols = gate_master.shape
    experts = all_experts // n_tp
    width = cols * n_tp // n_fs
    hidden, down_cols = down_master.shape[1], down_master.shape[2]
    any_spec = pl.BlockSpec(memory_space=pl.ANY)
    dma = pltpu.SemaphoreType.DMA
    up_shape = jax.ShapeDtypeStruct((experts, rows * n_gr * n_fs, width), BF16)
    return pl.pallas_call(
        functools.partial(exchange_kernel, n_gr, n_fs, n_tp),
        out_shape=(
            up_shape,
            up_shape,
            jax.ShapeDtypeStruct((experts, hidden, down_cols * n_gr * n_tp), BF16),
            jax.ShapeDtypeStruct((packed.shape[0], n_fs, *packed.shape[1:]), BF16),
        ),
        in_specs=[pl.BlockSpec(memory_space=pltpu.VMEM), *[any_spec] * 4],
        out_specs=(any_spec,) * 4,
        scratch_shapes=[
            pltpu.VMEM((2, n_tp, experts, rows, cols), BF16),
            pltpu.VMEM((n_tp, experts, hidden, down_cols), BF16),
            pltpu.VMEM((2, n_tp - 1, experts, rows, cols), BF16),
            pltpu.VMEM((2, n_tp, rows, cols), jnp.float32),
            pltpu.VMEM((n_tp, hidden, down_cols), jnp.float32),
            dma((2, n_tp)),
            dma((n_tp,)),
            dma((2, n_tp - 1, experts, n_fs // n_tp)),
            dma((2, n_tp - 1, experts, n_fs // n_tp)),
            dma((2, experts, n_fs)),
            dma((2, experts, n_fs)),
            dma((2, experts)),
            dma((2, experts, n_fs, n_gr - 1)),
            dma((2, experts, n_fs, n_gr - 1)),
            dma((n_tp - 1, experts)),
            dma((n_tp - 1, experts)),
            dma((experts,)),
            dma((experts, n_tp, n_gr - 1)),
            dma((experts, n_tp, n_gr - 1)),
            dma((4, n_fs // 2, experts)),
            dma((n_fs, experts)),
            dma,
        ],
        compiler_params=pltpu.CompilerParams(
            collective_id=0, has_side_effects=True, vmem_limit_bytes=52 * 1024 * 1024
        ),
        cost_estimate=pl.CostEstimate(flops=0, bytes_accessed=1_000_000_000, transcendentals=0),
    )(norm_gain[:, None], gate_master, up_master, down_master, packed)


def experts_kernel(
    slices, lead,
    pieces, gate_in, up_in, down_in,
    gate_out, up_out, down_out, sums,
    tall, wide, partial, gate_act, up_act, hidden,
    tall_load, tall_store, wide_load, wide_store,
):
    experts, features, width = gate_in.shape
    depth, cols = tall.shape[1], wide.shape[2]
    steps, ring = 2 * slices, tall.shape[0]
    count = hidden.shape[1]
    owners, tokens = sums.shape[0], sums.shape[1]
    ins, outs = (gate_in, up_in), (gate_out, up_out)

    def tall_ends(refs, e, j):
        return refs[j % 2].at[e, pl.ds(j // 2 * depth, depth)]

    def tall_slot(e, j):
        return lax.rem(e * steps + j, ring)

    def load_tall(e, j):
        slot = tall_slot(e, j)
        return pltpu.make_async_copy(tall_ends(ins, e, j), tall.at[slot], tall_load.at[slot])

    def store_tall(e, j):
        slot = tall_slot(e, j)
        return pltpu.make_async_copy(tall.at[slot], tall_ends(outs, e, j), tall_store.at[slot])

    def span(c):
        return pl.ds(pl.multiple_of(c * cols, cols), cols)

    def load_wide(c, e):
        slot = c * experts + e
        return pltpu.make_async_copy(down_in.at[e, :, span(c)], wide.at[slot], wide_load.at[slot])

    def store_wide(c, e):
        slot = c * experts + e
        return pltpu.make_async_copy(wide.at[slot], down_out.at[e, :, span(c)], wide_store.at[slot])

    for j in range(lead):
        load_tall(j // steps, j % steps).start()

    @pl.loop(0, experts)
    def _(e):
        for j in range(steps):
            load_tall(e, j).wait()
            store_tall(e, j).start()
            later, k = e + (j + lead) // steps, (j + lead) % steps

            @pl.when(later < experts)
            def _():
                @pl.when(later * steps + k >= ring)
                def _():
                    before = later * steps + k - ring
                    store_tall(before // steps, k).wait()

                load_tall(later, k).start()

            @pl.when(e == experts - 1)
            def _():
                for i in range(j, slices * experts // 2, steps):
                    load_wide(i // experts, i % experts).start()

            act = (gate_act, up_act)[j % 2]
            x = pieces[e, :, :, pl.ds(j // 2 * depth, depth)].reshape(count, depth)
            value = jnp.dot(x, tall[tall_slot(e, j)], preferred_element_type=jnp.float32)
            if j < 2:
                act[...] = value
            else:
                act[...] += value
        hidden[e] = (jax.nn.silu(gate_act[...]) * up_act[...]).astype(BF16)

    half = slices * experts // 2

    @pl.loop(0, slices)
    def _(c):
        for e in range(experts):
            load_wide(c, e).wait()
            store_wide(c, e).start()
            ahead = c * experts + e + half

            @pl.when(ahead < slices * experts)
            def _():
                load_wide(ahead // experts, lax.rem(ahead, experts)).start()

            value = jnp.dot(hidden[e], wide[c * experts + e], preferred_element_type=jnp.float32)
            partial[e] = value.astype(BF16).reshape(partial.shape[1:])

        for o in range(owners):
            weights = pieces[:, o, :, pl.ds(features, tokens)].reshape(-1, tokens)
            rows = partial[:, o].reshape(-1, cols)
            sums[o, :, span(c)] = lax.dot_general(
                weights, rows, (((0,), (0,)), ((), ())), preferred_element_type=jnp.float32
            ).astype(BF16)

    for i in range(ring):
        at = experts * steps - ring + i
        store_tall(at // steps, at % steps).wait()
    for c in range(slices):
        for e in range(experts):
            store_wide(c, e).wait()


def run_experts(pieces, gate, up, down):
    experts, features, width = gate.shape
    _, owners, cap, padded = pieces.shape
    tokens, count, slices = padded - features, owners * cap, 4
    ring = 2 * 2 * slices
    any_spec = pl.BlockSpec(memory_space=pl.ANY)
    vmem = pl.BlockSpec(memory_space=pltpu.VMEM)
    dma = pltpu.SemaphoreType.DMA
    return pl.pallas_call(
        functools.partial(experts_kernel, slices, 2 * slices),
        out_shape=(
            jax.ShapeDtypeStruct(gate.shape, BF16),
            jax.ShapeDtypeStruct(up.shape, BF16),
            jax.ShapeDtypeStruct(down.shape, BF16),
            jax.ShapeDtypeStruct((owners, tokens, features), BF16),
        ),
        in_specs=[vmem, any_spec, any_spec, any_spec],
        out_specs=(any_spec, any_spec, any_spec, vmem),
        scratch_shapes=[
            pltpu.VMEM((ring, features // slices, width), BF16),
            pltpu.VMEM((slices * experts, width, features // slices), BF16),
            pltpu.VMEM((experts, owners, cap, features // slices), BF16),
            pltpu.VMEM((count, width), jnp.float32),
            pltpu.VMEM((count, width), jnp.float32),
            pltpu.VMEM((experts, count, width), BF16),
            dma((ring,)),
            dma((ring,)),
            dma((slices * experts,)),
            dma((slices * experts,)),
        ],
        compiler_params=pltpu.CompilerParams(vmem_limit_bytes=44 * 1024 * 1024),
        cost_estimate=pl.CostEstimate(
            flops=6 * experts * count * features * width,
            bytes_accessed=12 * experts * features * width, transcendentals=0,
        ),
    )(pieces, gate, up, down)


def plan_of(n_bits, features):
    rest = list(range(2, n_bits))
    orders = ([0, "x", 1, *rest], ["x", 1, 0, *rest], [1, 0, "x", *rest])
    unit = 128
    units = features // unit
    shares, chunks, begin = [], [], 0
    for i in range(6):
        shares.append((units - sum(shares)) // (6 - i))
    for i, share in enumerate(shares):
        if share:
            chunks.append((orders[i % 3], begin * unit, share * unit))
        begin += share
    return chunks


def combine_kernel(n_fs, chunks, sums, out, acc, *rest):
    stages = len(chunks[0][0])
    boxes, (s_send, s_recv, o_send, o_recv) = rest[:-4], rest[-4:]
    gr, fs, tp = (lax.axis_index(name) for name in ("gr", "fs", "tp"))
    n_bits = stages - 1
    rows = sums.shape[-2]
    bits = [lax.rem(fs // (1 << b), 2) for b in range(n_bits)]

    def mine(dim):
        return tp if dim == "x" else bits[dim]

    def partner(dim):
        if dim == "x":
            return (gr, fs, 1 - tp)
        return (gr, fs + (1 - 2 * bits[dim]) * (1 << dim), tp)

    def block(order, stage, own, cols):
        index = [slice(None)] * (n_bits + 1)
        for dim in order[: stage + 1]:
            at = n_bits if dim == "x" else n_bits - 1 - dim
            index[at] = mine(dim)
            if dim == order[stage] and not own:
                index[at] = 1 - mine(dim)
        return (*index, slice(None), cols)

    barrier = pltpu.get_barrier_semaphore()
    for dim in [*range(n_bits), "x"]:
        pl.semaphore_signal(barrier, 1, device_id=partner(dim), device_id_type=MESH)
    pl.semaphore_wait(barrier, n_bits + 1)

    def step(i, stage):
        order, begin, size = chunks[i]
        held = sums if stage == 0 else acc
        return pltpu.make_async_remote_copy(
            held.at[block(order, stage, False, pl.ds(begin, size))],
            boxes[i * stages + stage], s_send.at[i, stage], s_recv.at[i, stage],
            device_id=partner(order[stage]), device_id_type=MESH,
        )

    def finished(i):
        _, begin, size = chunks[i]
        here = out.at[pl.ds(pl.multiple_of(tp * rows, rows), rows), pl.ds(begin, size)]
        return pltpu.make_async_remote_copy(
            here, here, o_send.at[i], o_recv.at[i], device_id=partner("x"), device_id_type=MESH
        )

    for i in range(len(chunks)):
        step(i, 0).start()
    for stage in range(stages):
        for i, (order, begin, size) in enumerate(chunks):
            step(i, stage).wait_recv()
            at = block(order, stage, True, pl.ds(begin, size))
            held = sums if stage == 0 else acc
            value = held[at].astype(jnp.float32) + boxes[i * stages + stage][...].astype(jnp.float32)
            if stage + 1 < stages:
                acc[at] = value.astype(BF16)
                step(i, stage + 1).start()
            else:
                out[pl.ds(pl.multiple_of(tp * rows, rows), rows), pl.ds(begin, size)] = value.astype(BF16)
                finished(i).start()
    for i in range(len(chunks)):
        _, begin, size = chunks[i]
        there = out.at[pl.ds(pl.multiple_of((1 - tp) * rows, rows), rows), pl.ds(begin, size)]
        pltpu.make_async_remote_copy(
            there, there, o_send.at[i], o_recv.at[i], device_id=partner("x"), device_id_type=MESH
        ).wait_recv()
        finished(i).wait_send()
        for stage in range(stages):
            step(i, stage).wait_send()


def combine(n_fs, sums):
    owners, tokens, features = sums.shape
    n_bits = n_fs.bit_length() - 1
    stages, rows = n_bits + 1, tokens // 2
    chunks = plan_of(n_bits, features)
    dma = pltpu.SemaphoreType.DMA
    vmem = pl.BlockSpec(memory_space=pltpu.VMEM)
    boxes = [
        pltpu.VMEM((*(2,) * (n_bits - stage), rows, size), BF16)
        for _, _, size in chunks for stage in range(stages)
    ]
    view = (*(2,) * (n_bits + 1), rows, features)
    return pl.pallas_call(
        functools.partial(combine_kernel, n_fs, chunks),
        out_shape=jax.ShapeDtypeStruct((tokens, features), BF16),
        in_specs=[vmem],
        out_specs=vmem,
        scratch_shapes=[
            pltpu.VMEM(view, BF16),
            *boxes,
            dma((len(chunks), stages)),
            dma((len(chunks), stages)),
            dma((len(chunks),)),
            dma((len(chunks),)),
        ],
        compiler_params=pltpu.CompilerParams(
            collective_id=1, has_side_effects=True, vmem_limit_bytes=40 * 1024 * 1024
        ),
    )(sums.reshape(view))


def plain_local(tokens, route_ids, route_logits, norm_gain, gate_master, up_master, down_master):
    gain_rows = norm_gain[None, :, None]
    gate_half = (gate_master * gain_rows).astype(jnp.bfloat16)
    up_half = (up_master * gain_rows).astype(jnp.bfloat16)
    down_half = down_master.astype(jnp.bfloat16)
    gate_cols, up_cols, down_cols = (
        lax.all_to_all(gate_half, "tp", split_axis=0, concat_axis=2, tiled=True),
        lax.all_to_all(up_half, "tp", split_axis=0, concat_axis=2, tiled=True),
        lax.all_to_all(down_half, "tp", split_axis=0, concat_axis=2, tiled=True),
    )
    gate_part, up_part = (
        lax.all_to_all(gate_cols, "fs", split_axis=2, concat_axis=1, tiled=True),
        lax.all_to_all(up_cols, "fs", split_axis=2, concat_axis=1, tiled=True),
    )
    gate_weight, up_weight, down_weight = (
        lax.all_gather(gate_part, "gr", axis=1, tiled=True),
        lax.all_gather(up_part, "gr", axis=1, tiled=True),
        lax.all_gather(down_cols, "gr", axis=2, tiled=True),
    )
    as_float = tokens.astype(jnp.float32)
    normed = (
        as_float * lax.rsqrt(jnp.mean(as_float * as_float, axis=-1, keepdims=True) + epsilon)
    ).astype(jnp.bfloat16)
    differ = route_logits[:, 0] - route_logits[:, 1]
    route_weight = jnp.stack([jax.nn.sigmoid(differ), jax.nn.sigmoid(-differ)], axis=1)
    experts_here = gate_weight.shape[0]
    first_expert = lax.axis_index("tp") * experts_here
    expert_ids = first_expert + jnp.arange(experts_here, dtype=jnp.int32)
    route_hits = route_ids[None, :, :] == expert_ids[:, None, None]
    chosen = jnp.any(route_hits, axis=2)
    weight_rows = jnp.sum(jnp.where(route_hits, route_weight[None, :, :], 0.0), axis=2)
    slot_rank = jnp.cumsum(chosen.astype(jnp.int32), axis=1) - 1
    slot_ids = jnp.arange(CAP, dtype=jnp.int32)
    picker = chosen[:, None, :] & (slot_rank[:, None, :] == slot_ids[None, :, None])
    picker_float = picker.astype(jnp.float32)
    packed = jnp.einsum(
        "xsr,rd->sxd", picker.astype(jnp.bfloat16), normed, preferred_element_type=jnp.float32
    ).astype(jnp.bfloat16)
    slot_weight = jnp.einsum(
        "xsr,xr->sx", picker_float, weight_rows, precision=lax.Precision.HIGHEST
    )
    pieces = lax.all_gather(packed, "fs", axis=0, tiled=True)
    gate_act = jnp.einsum("kxd,xdh->kxh", pieces, gate_weight, preferred_element_type=jnp.float32)
    up_act = jnp.einsum("kxd,xdh->kxh", pieces, up_weight, preferred_element_type=jnp.float32)
    hidden = (jax.nn.silu(gate_act) * up_act).astype(jnp.bfloat16)
    expert_out = lax.psum_scatter(
        jnp.einsum("kxh,xhd->kxd", hidden, down_weight, preferred_element_type=jnp.float32).astype(
            jnp.bfloat16
        ),
        "fs",
        scatter_dimension=0,
        tiled=True,
    ).astype(jnp.float32)
    weighted = expert_out * slot_weight[:, :, None]
    block_sum = jnp.einsum("xsr,sxd->rd", picker_float, weighted, precision=lax.Precision.HIGHEST)
    mixed = lax.psum(block_sum.astype(jnp.bfloat16), "tp")
    return (gate_weight, up_weight, down_weight, mixed)


def fast_local(sizes, tokens, route_ids, route_logits, norm_gain, gate_master, up_master, down_master):
    n_gr, n_fs, n_tp = sizes
    as_float = tokens.astype(jnp.float32)
    normed = (
        as_float * lax.rsqrt(jnp.mean(as_float * as_float, axis=-1, keepdims=True) + epsilon)
    ).astype(jnp.bfloat16)
    differ = route_logits[:, 0] - route_logits[:, 1]
    route_weight = jnp.stack([jax.nn.sigmoid(differ), jax.nn.sigmoid(-differ)], axis=1)
    experts_here = gate_master.shape[0] // n_tp
    first_expert = lax.axis_index("tp") * experts_here
    expert_ids = first_expert + jnp.arange(experts_here, dtype=jnp.int32)
    route_hits = route_ids[None, :, :] == expert_ids[:, None, None]
    chosen = jnp.any(route_hits, axis=2)
    weight_rows = jnp.sum(jnp.where(route_hits, route_weight[None, :, :], 0.0), axis=2)
    slot_rank = jnp.cumsum(chosen.astype(jnp.int32), axis=1) - 1
    slot_ids = jnp.arange(CAP, dtype=jnp.int32)
    picker = chosen[:, None, :] & (slot_rank[:, None, :] == slot_ids[None, :, None])
    packed = jnp.einsum(
        "xsr,rd->xsd", picker.astype(jnp.bfloat16), normed, preferred_element_type=jnp.float32
    ).astype(jnp.bfloat16)
    combiner = (picker.astype(jnp.float32) * weight_rows[:, None, :]).astype(jnp.bfloat16)
    gate_moved, up_moved, down_moved, pieces = exchange(
        sizes, norm_gain, gate_master, up_master, down_master,
        jnp.concatenate([packed, combiner], axis=2),
    )
    gate_weight, up_weight, down_weight, sums = run_experts(
        pieces, gate_moved, up_moved, down_moved
    )
    return (gate_weight, up_weight, down_weight, combine(n_fs, sums))


def solution(mesh):
    n_gr, n_fs, n_tp = (mesh.shape[name] for name in ("gr", "fs", "tp"))
    placed = (
        P(("gr", "fs"), None),
        P(("gr", "fs"), None),
        P(("gr", "fs"), None),
        P(("gr", "fs")),
        P(None, ("gr", "fs"), "tp"),
        P(None, ("gr", "fs"), "tp"),
        P(None, "fs", ("gr", "tp")),
    )

    def local(tokens, route_ids, route_logits, norm_gain, gate_master, up_master, down_master):
        width = gate_master.shape[2] * n_tp // n_fs
        aligned = width % 128 == 0 and down_master.shape[2] % 128 == 0
        fits = n_fs % n_tp == 0 and n_fs & (n_fs - 1) == 0 and n_fs > 2
        fits = fits and n_gr > 1 and n_tp == 2 and tokens.shape[0] % 128 == 0
        run = functools.partial(fast_local, (n_gr, n_fs, n_tp)) if aligned and fits else plain_local
        return run(tokens, route_ids, route_logits, norm_gain, gate_master, up_master, down_master)

    return jax.shard_map(
        local,
        mesh=mesh,
        in_specs=placed,
        out_specs=(
            P("tp", None, "fs"),
            P("tp", None, "fs"),
            P("tp", "fs", None),
            P(("gr", "fs"), None),
        ),
        check_vma=False,
    )
```

```python
import functools

import jax
import jax.numpy as jnp
from jax import lax
from jax.experimental import pallas as pl
from jax.experimental.pallas import tpu as pltpu
from jax.sharding import PartitionSpec as P

CAP = 32


epsilon = 1e-06
MESH = pl.DeviceIdType.MESH
BF16 = jnp.bfloat16


def exchange_kernel(
    n_gr, n_fs, n_tp,
    gain_ref, gate_ref, up_ref, down_ref, packed_ref,
    gate_out, up_out, down_out, pieces,
    stage, stage_down, crossed, raw, raw_down,
    load_sem, load_down_sem, x_send, x_recv, s_send, s_recv, own_sem,
    d_send, d_recv, xd_send, xd_recv, own_down_sem, dd_send, dd_recv,
    p_send, p_recv, p_own, q_send, q_recv,
):
    gr, fs, tp = (lax.axis_index(name) for name in ("gr", "fs", "tp"))
    experts, _, width = gate_out.shape
    rows, cols = gate_ref.shape[1], gate_ref.shape[2]
    per = cols // width
    down_cols = down_ref.shape[2]
    masters, outs = (gate_ref, up_ref), (gate_out, up_out)

    barrier = pltpu.get_barrier_semaphore()
    peers = 0
    for o in range(1, n_tp):
        pl.semaphore_signal(barrier, 1, device_id=(gr, fs, lax.rem(tp + o, n_tp)), device_id_type=MESH)
        peers += 1
    for k in range(1, n_fs):
        pl.semaphore_signal(barrier, 1, device_id=(gr, lax.rem(fs + k, n_fs), tp), device_id_type=MESH)
        peers += 1
    for o in range(1, n_gr):
        pl.semaphore_signal(barrier, 1, device_id=(lax.rem(gr + o, n_gr), fs, tp), device_id_type=MESH)
        peers += 1

    def tp_at(o):
        return lax.rem(tp + o, n_tp)

    order = [(w, o) for w in range(2) for o in [*range(1, n_tp), 0]]

    def load(e, w, o):
        return pltpu.make_async_copy(
            masters[w].at[tp_at(o) * experts + e], raw.at[w, o], load_sem.at[w, o]
        )

    def load_down(e, o):
        return pltpu.make_async_copy(
            down_ref.at[tp_at(o) * experts + e], raw_down.at[o], load_down_sem.at[o]
        )

    def over_tp(e, w, o, j):
        columns = pl.ds(j * width, width)
        return pltpu.make_async_remote_copy(
            stage.at[w, o, e, :, columns], crossed.at[w, o - 1, e, :, columns],
            x_send.at[w, o - 1, e, j], x_recv.at[w, o - 1, e, j],
            device_id=(gr, fs, tp_at(o)), device_id_type=MESH,
        )

    def rows_of(group, owner):
        return pl.ds(pl.multiple_of((group * n_fs + owner) * rows, rows), rows)

    def source(e, w, o, j):
        columns = pl.ds(j * width, width)
        if o == 0:
            return stage.at[w, 0, e, :, columns]
        return crossed.at[w, o - 1, e, :, columns]

    def fan(e, w, o):
        begin = lax.rem(tp - o + n_tp, n_tp) * per
        for j in range(per):
            if o:
                over_tp(e, w, o, j).wait_recv()
            to = begin + j
            k = lax.rem(to - fs + n_fs, n_fs)
            target = outs[w].at[e, rows_of(gr, fs)]

            @pl.when(to != fs)
            def _():
                pltpu.make_async_remote_copy(
                    source(e, w, o, j), target, s_send.at[w, e, k], s_recv.at[w, e, k],
                    device_id=(gr, to, tp), device_id_type=MESH,
                ).start()

            @pl.when(to == fs)
            def _():
                pltpu.make_async_copy(source(e, w, o, j), target, own_sem.at[w, e]).start()

    def arrival(e, w, k):
        piece = outs[w].at[e, rows_of(gr, lax.rem(fs - k + n_fs, n_fs))]
        return pltpu.make_async_remote_copy(
            piece, piece, s_send.at[w, e, k], s_recv.at[w, e, k],
            device_id=(gr, lax.rem(fs + k, n_fs), tp), device_id_type=MESH,
        )

    def own_copy(e, w):
        return pltpu.make_async_copy(
            source(e, w, 0, 0), outs[w].at[e, rows_of(gr, fs)], own_sem.at[w, e]
        )

    def over_gr(e, w, k, o, group):
        piece = outs[w].at[e, rows_of(group, lax.rem(fs - k + n_fs, n_fs))]
        return pltpu.make_async_remote_copy(
            piece, piece, d_send.at[w, e, k, o - 1], d_recv.at[w, e, k, o - 1],
            device_id=(lax.rem(gr + o, n_gr), fs, tp), device_id_type=MESH,
        )

    def down_block(group, t):
        return pl.ds(pl.multiple_of((group * n_tp + t) * down_cols, down_cols), down_cols)

    def down_over_tp(e, o):
        return pltpu.make_async_remote_copy(
            stage_down.at[o, e], down_out.at[e, :, down_block(gr, tp)],
            xd_send.at[o - 1, e], xd_recv.at[o - 1, e],
            device_id=(gr, fs, tp_at(o)), device_id_type=MESH,
        )

    def down_arrival(e, o):
        piece = down_out.at[e, :, down_block(gr, lax.rem(tp - o + n_tp, n_tp))]
        return pltpu.make_async_remote_copy(
            piece, piece, xd_send.at[o - 1, e], xd_recv.at[o - 1, e],
            device_id=(gr, fs, tp_at(o)), device_id_type=MESH,
        )

    def down_own(e):
        return pltpu.make_async_copy(
            stage_down.at[0, e], down_out.at[e, :, down_block(gr, tp)], own_down_sem.at[e]
        )

    def down_over_gr(e, s, o, group):
        piece = down_out.at[e, :, down_block(group, lax.rem(tp - s + n_tp, n_tp))]
        return pltpu.make_async_remote_copy(
            piece, piece, dd_send.at[e, s, o - 1], dd_recv.at[e, s, o - 1],
            device_id=(lax.rem(gr + o, n_gr), fs, tp), device_id_type=MESH,
        )

    pairs = n_fs // 2
    z, y = fs // 2, lax.rem(fs, 2)

    depth = packed_ref.shape[0] // experts
    share = packed_ref.shape[1] - packed_ref.shape[0]

    def strip(e):
        return pl.ds(e * depth, depth)

    def relay(kind, hop, e):
        at = {"up": z - hop, "down": z + hop, "over": z - hop, "over_down": z + hop}[kind]
        to = {"up": fs + 2, "down": fs - 2}.get(kind, fs + 1 - 2 * y)
        origin = at * 2 + y
        here = packed_ref.at[strip(e)] if hop == 0 else pieces.at[tp, origin, strip(e)]
        slot = ["up", "down", "over", "over_down"].index(kind)
        return pltpu.make_async_remote_copy(
            here, pieces.at[tp, origin, strip(e)], p_send.at[slot, hop, e], p_recv.at[origin, e],
            device_id=(gr, to, tp), device_id_type=MESH,
        )

    def landed(origin, e):
        piece = pieces.at[tp, origin, strip(e)]
        return pltpu.make_async_remote_copy(
            piece, piece, p_send.at[0, 0, e], p_recv.at[origin, e],
            device_id=(gr, fs + 1 - 2 * y, tp), device_id_type=MESH,
        )

    def relayed(kind, hop):
        if kind == "up":
            return (z - hop >= 0) & (z + 1 < pairs)
        if kind == "down":
            return (z + hop < pairs) & (z >= 1)
        return z - hop >= 0 if kind == "over" else z + hop < pairs

    def relay_start(kind, hop, e):
        @pl.when(relayed(kind, hop))
        def _():
            relay(kind, hop, e).start()

    def relay_from(hop):
        for e in range(experts):
            @pl.when(z - hop >= 0)
            def _():
                landed((z - hop) * 2 + y, e).wait_recv()

            relay_start("up", hop, e)
            relay_start("over", hop, e)

            @pl.when(z + hop < pairs)
            def _():
                landed((z + hop) * 2 + y, e).wait_recv()

            relay_start("down", hop, e)
            relay_start("over_down", hop, e)

    own_piece = pltpu.make_async_copy(packed_ref, pieces.at[tp, fs], p_own)

    def across(origin, side):
        part = pieces.at[side, origin, :, pl.ds(0, share)]
        return pltpu.make_async_remote_copy(
            part, part, q_send.at[origin], q_recv.at[origin],
            device_id=(gr, fs, tp_at(1)), device_id_type=MESH,
        )

    for w, o in order:
        load(0, w, o).start()
    for o in range(n_tp):
        load_down(0, o).start()
    pl.semaphore_wait(barrier, peers)
    for kind in ("up", "down", "over"):
        for e in range(experts):
            relay_start(kind, 0, e)
    own_piece.start()

    def cast(e, leg):
        for w, o in order:
            if (o > 0) != (leg == "tp"):
                continue
            load(e, w, o).wait()
            stage[w, o, e] = (raw[w, o] * gain_ref[...]).astype(BF16)

            @pl.when(e + 1 < experts)
            def _():
                load(e + 1, w, o).start()

            if o:
                for j in range(per):
                    over_tp(e, w, o, j).start()
            else:
                fan(e, w, 0)

    def forward(e):
        for w in range(2):
            for o in range(1, n_tp):
                fan(e, w, o)

    cast(0, "tp")
    for hop in range(1, pairs):
        relay_from(hop)
    cast(0, "fs")

    @pl.loop(1, experts)
    def _(e):
        cast(e, "tp")
        cast(e, "fs")
        forward(e - 1)

    own_piece.wait()
    for at in range(pairs):
        for e in range(experts):
            landed(at * 2 + 1 - y, e).wait_recv()

    @pl.loop(0, n_fs)
    def _(origin):
        across(origin, tp).start()

    @pl.loop(0, experts)
    def _(e):
        for o in [*range(1, n_tp), 0]:
            load_down(e, o).wait()
            stage_down[o, e] = raw_down[o].astype(BF16)

            @pl.when(e + 1 < experts)
            def _():
                load_down(e + 1, o).start()

            if o:
                down_over_tp(e, o).start()
            else:
                down_own(e).start()

    def collect(e):
        for w in range(2):
            own_copy(e, w).wait()
            for o in range(1, n_gr):
                over_gr(e, w, 0, o, gr).start()

        @pl.loop(1, n_fs)
        def _(k):
            for w in range(2):
                arrival(e, w, k).wait_recv()
                for o in range(1, n_gr):
                    over_gr(e, w, k, o, gr).start()

    forward(experts - 1)

    @pl.loop(0, experts - 1)
    def _(e):
        collect(e)

    @pl.loop(0, experts)
    def _(e):
        down_own(e).wait()
        for s in range(1, n_tp):
            down_arrival(e, s).wait_recv()
        for s in range(n_tp):
            for o in range(1, n_gr):
                down_over_gr(e, s, o, gr).start()

    collect(experts - 1)

    @pl.loop(0, experts)
    def _(e):
        for w in range(2):
            for o in range(1, n_tp):
                for j in range(per):
                    over_tp(e, w, o, j).wait_send()

            @pl.loop(1, n_fs)
            def _(k):
                arrival(e, w, k).wait_send()

            @pl.loop(0, n_fs)
            def _(k):
                for o in range(1, n_gr):
                    over_gr(e, w, k, o, gr).wait_send()
                    over_gr(e, w, k, o, lax.rem(gr - o + n_gr, n_gr)).wait_recv()

        for s in range(1, n_tp):
            down_over_tp(e, s).wait_send()
        for s in range(n_tp):
            for o in range(1, n_gr):
                down_over_gr(e, s, o, gr).wait_send()
                down_over_gr(e, s, o, lax.rem(gr - o + n_gr, n_gr)).wait_recv()

    @pl.loop(0, n_fs)
    def _(origin):
        across(origin, tp).wait_send()
        across(origin, 1 - tp).wait_recv()

    for kind in ("up", "down", "over", "over_down"):
        for hop in range(1 if kind == "over_down" else 0, pairs):
            @pl.when(relayed(kind, hop))
            def _():
                for e in range(experts):
                    relay(kind, hop, e).wait_send()


def exchange(sizes, norm_gain, gate_master, up_master, down_master, packed):
    n_gr, n_fs, n_tp = sizes
    all_experts, rows, cols = gate_master.shape
    experts = all_experts // n_tp
    width = cols * n_tp // n_fs
    hidden, down_cols = down_master.shape[1], down_master.shape[2]
    any_spec = pl.BlockSpec(memory_space=pl.ANY)
    dma = pltpu.SemaphoreType.DMA
    up_shape = jax.ShapeDtypeStruct((experts, rows * n_gr * n_fs, width), BF16)
    return pl.pallas_call(
        functools.partial(exchange_kernel, n_gr, n_fs, n_tp),
        out_shape=(
            up_shape,
            up_shape,
            jax.ShapeDtypeStruct((experts, hidden, down_cols * n_gr * n_tp), BF16),
            jax.ShapeDtypeStruct((n_tp, n_fs, *packed.shape), BF16),
        ),
        in_specs=[pl.BlockSpec(memory_space=pltpu.VMEM), *[any_spec] * 4],
        out_specs=(any_spec,) * 4,
        scratch_shapes=[
            pltpu.VMEM((2, n_tp, experts, rows, cols), BF16),
            pltpu.VMEM((n_tp, experts, hidden, down_cols), BF16),
            pltpu.VMEM((2, n_tp - 1, experts, rows, cols), BF16),
            pltpu.VMEM((2, n_tp, rows, cols), jnp.float32),
            pltpu.VMEM((n_tp, hidden, down_cols), jnp.float32),
            dma((2, n_tp)),
            dma((n_tp,)),
            dma((2, n_tp - 1, experts, n_fs // n_tp)),
            dma((2, n_tp - 1, experts, n_fs // n_tp)),
            dma((2, experts, n_fs)),
            dma((2, experts, n_fs)),
            dma((2, experts)),
            dma((2, experts, n_fs, n_gr - 1)),
            dma((2, experts, n_fs, n_gr - 1)),
            dma((n_tp - 1, experts)),
            dma((n_tp - 1, experts)),
            dma((experts,)),
            dma((experts, n_tp, n_gr - 1)),
            dma((experts, n_tp, n_gr - 1)),
            dma((4, n_fs // 2, experts)),
            dma((n_fs, experts)),
            dma,
            dma((n_fs,)),
            dma((n_fs,)),
        ],
        compiler_params=pltpu.CompilerParams(
            collective_id=0, has_side_effects=True, vmem_limit_bytes=52 * 1024 * 1024
        ),
        cost_estimate=pl.CostEstimate(flops=0, bytes_accessed=1_000_000_000, transcendentals=0),
    )(norm_gain[:, None], gate_master, up_master, down_master, packed)


def experts_kernel(
    slices, lead,
    blocks, gate_in, up_in, down_in,
    gate_out, up_out, down_out, sums,
    tall, wide, pieces, partial, gate_act, up_act, hidden,
    tall_load, tall_store, wide_load, wide_store,
):
    experts, features, width = gate_in.shape
    depth, cols = tall.shape[1], wide.shape[2]
    steps, ring = 2 * slices, tall.shape[0]
    count = hidden.shape[1]
    owners, tokens = sums.shape[0], sums.shape[1]
    ins, outs = (gate_in, up_in), (gate_out, up_out)

    def tall_ends(refs, e, j):
        return refs[j % 2].at[e, pl.ds(j // 2 * depth, depth)]

    def tall_slot(e, j):
        return lax.rem(e * steps + j, ring)

    def load_tall(e, j):
        slot = tall_slot(e, j)
        return pltpu.make_async_copy(tall_ends(ins, e, j), tall.at[slot], tall_load.at[slot])

    def store_tall(e, j):
        slot = tall_slot(e, j)
        return pltpu.make_async_copy(tall.at[slot], tall_ends(outs, e, j), tall_store.at[slot])

    def span(c):
        return pl.ds(pl.multiple_of(c * cols, cols), cols)

    def load_wide(c, e):
        slot = c * experts + e
        return pltpu.make_async_copy(down_in.at[e, :, span(c)], wide.at[slot], wide_load.at[slot])

    def store_wide(c, e):
        slot = c * experts + e
        return pltpu.make_async_copy(wide.at[slot], down_out.at[e, :, span(c)], wide_store.at[slot])

    for j in range(lead):
        load_tall(j // steps, j % steps).start()

    tp = lax.axis_index("tp")
    share = blocks.shape[3] - tokens

    @pl.loop(0, owners)
    def _(o):
        picker = (blocks[tp, o, :, pl.ds(share, tokens)].astype(jnp.float32) > 0).astype(BF16)
        for side in range(blocks.shape[0]):
            rows = jnp.dot(
                picker, blocks[side, o, :, pl.ds(0, share)], preferred_element_type=jnp.float32
            ).astype(BF16)
            pieces[:, o, :, pl.ds(side * share, share)] = rows.reshape(experts, -1, share)

    @pl.loop(0, experts)
    def _(e):
        for j in range(steps):
            load_tall(e, j).wait()
            store_tall(e, j).start()
            later, k = e + (j + lead) // steps, (j + lead) % steps

            @pl.when(later < experts)
            def _():
                @pl.when(later * steps + k >= ring)
                def _():
                    before = later * steps + k - ring
                    store_tall(before // steps, k).wait()

                load_tall(later, k).start()

            @pl.when(e == experts - 1)
            def _():
                for i in range(j, slices * experts // 2, steps):
                    load_wide(i // experts, i % experts).start()

            act = (gate_act, up_act)[j % 2]
            x = pieces[e, :, :, pl.ds(j // 2 * depth, depth)].reshape(count, depth)
            value = jnp.dot(x, tall[tall_slot(e, j)], preferred_element_type=jnp.float32)
            if j < 2:
                act[...] = value
            else:
                act[...] += value
        hidden[e] = (jax.nn.silu(gate_act[...]) * up_act[...]).astype(BF16)

    half = slices * experts // 2

    @pl.loop(0, slices)
    def _(c):
        for e in range(experts):
            load_wide(c, e).wait()
            store_wide(c, e).start()
            ahead = c * experts + e + half

            @pl.when(ahead < slices * experts)
            def _():
                load_wide(ahead // experts, lax.rem(ahead, experts)).start()

            value = jnp.dot(hidden[e], wide[c * experts + e], preferred_element_type=jnp.float32)
            partial[e] = value.astype(BF16).reshape(partial.shape[1:])

        for o in range(owners):
            weights = blocks[tp, o, :, pl.ds(share, tokens)]
            rows = partial[:, o].reshape(-1, cols)
            sums[o, :, span(c)] = lax.dot_general(
                weights, rows, (((0,), (0,)), ((), ())), preferred_element_type=jnp.float32
            ).astype(BF16)

    for i in range(ring):
        at = experts * steps - ring + i
        store_tall(at // steps, at % steps).wait()
    for c in range(slices):
        for e in range(experts):
            store_wide(c, e).wait()


def run_experts(blocks, gate, up, down):
    experts, features, width = gate.shape
    _, owners, tokens, _ = blocks.shape
    cap, slices = tokens // experts, 4
    count = owners * cap
    ring = 2 * 2 * slices
    any_spec = pl.BlockSpec(memory_space=pl.ANY)
    vmem = pl.BlockSpec(memory_space=pltpu.VMEM)
    dma = pltpu.SemaphoreType.DMA
    return pl.pallas_call(
        functools.partial(experts_kernel, slices, 3 * slices),
        out_shape=(
            jax.ShapeDtypeStruct(gate.shape, BF16),
            jax.ShapeDtypeStruct(up.shape, BF16),
            jax.ShapeDtypeStruct(down.shape, BF16),
            pltpu.VMEM((owners, tokens, features), BF16),
        ),
        in_specs=[vmem, any_spec, any_spec, any_spec],
        out_specs=(any_spec, any_spec, any_spec, vmem),
        scratch_shapes=[
            pltpu.VMEM((ring, features // slices, width), BF16),
            pltpu.VMEM((slices * experts, width, features // slices), BF16),
            pltpu.VMEM((experts, owners, cap, features), BF16),
            pltpu.VMEM((experts, owners, cap, features // slices), BF16),
            pltpu.VMEM((count, width), jnp.float32),
            pltpu.VMEM((count, width), jnp.float32),
            pltpu.VMEM((experts, count, width), BF16),
            dma((ring,)),
            dma((ring,)),
            dma((slices * experts,)),
            dma((slices * experts,)),
        ],
        compiler_params=pltpu.CompilerParams(vmem_limit_bytes=50 * 1024 * 1024),
        cost_estimate=pl.CostEstimate(
            flops=6 * experts * count * features * width,
            bytes_accessed=12 * experts * features * width, transcendentals=0,
        ),
    )(blocks, gate, up, down)


def plan_of(n_bits, features):
    rest = list(range(2, n_bits))
    orders = ([0, "x", 1, *rest], ["x", 1, 0, *rest], [1, 0, "x", *rest])
    unit = 128
    units = features // unit
    shares, chunks, begin = [], [], 0
    for i in range(6):
        shares.append(-((sum(shares) - units) // (6 - i)))
    for i, share in enumerate(shares):
        if share:
            chunks.append((orders[i % 3], begin * unit, share * unit))
        begin += share
    return chunks


def combine_kernel(n_fs, chunks, sums, out, acc, *rest):
    stages = len(chunks[0][0])
    boxes, (s_send, s_recv, o_send, o_recv) = rest[:-4], rest[-4:]
    gr, fs, tp = (lax.axis_index(name) for name in ("gr", "fs", "tp"))
    n_bits = stages - 1
    rows = sums.shape[-2]
    bits = [lax.rem(fs // (1 << b), 2) for b in range(n_bits)]

    def mine(dim):
        return tp if dim == "x" else bits[dim]

    def partner(dim):
        if dim == "x":
            return (gr, fs, 1 - tp)
        return (gr, fs + (1 - 2 * bits[dim]) * (1 << dim), tp)

    def block(order, stage, own, cols):
        index = [slice(None)] * (n_bits + 1)
        for dim in order[: stage + 1]:
            at = n_bits if dim == "x" else n_bits - 1 - dim
            index[at] = mine(dim)
            if dim == order[stage] and not own:
                index[at] = 1 - mine(dim)
        return (*index, slice(None), cols)

    barrier = pltpu.get_barrier_semaphore()
    for dim in [*range(n_bits), "x"]:
        pl.semaphore_signal(barrier, 1, device_id=partner(dim), device_id_type=MESH)
    pl.semaphore_wait(barrier, n_bits + 1)

    def step(i, stage):
        order, begin, size = chunks[i]
        held = sums if stage == 0 else acc
        return pltpu.make_async_remote_copy(
            held.at[block(order, stage, False, pl.ds(begin, size))],
            boxes[i * stages + stage], s_send.at[i, stage], s_recv.at[i, stage],
            device_id=partner(order[stage]), device_id_type=MESH,
        )

    def finished(i):
        _, begin, size = chunks[i]
        here = out.at[pl.ds(pl.multiple_of(tp * rows, rows), rows), pl.ds(begin, size)]
        return pltpu.make_async_remote_copy(
            here, here, o_send.at[i], o_recv.at[i], device_id=partner("x"), device_id_type=MESH
        )

    for i in range(len(chunks)):
        step(i, 0).start()
    for stage in range(stages):
        for i, (order, begin, size) in enumerate(chunks):
            step(i, stage).wait_recv()
            at = block(order, stage, True, pl.ds(begin, size))
            held = sums if stage == 0 else acc
            value = held[at].astype(jnp.float32) + boxes[i * stages + stage][...].astype(jnp.float32)
            if stage + 1 < stages:
                acc[at] = value.astype(BF16)
                step(i, stage + 1).start()
            else:
                out[pl.ds(pl.multiple_of(tp * rows, rows), rows), pl.ds(begin, size)] = value.astype(BF16)
                finished(i).start()
    for i in range(len(chunks)):
        _, begin, size = chunks[i]
        there = out.at[pl.ds(pl.multiple_of((1 - tp) * rows, rows), rows), pl.ds(begin, size)]
        pltpu.make_async_remote_copy(
            there, there, o_send.at[i], o_recv.at[i], device_id=partner("x"), device_id_type=MESH
        ).wait_recv()
        finished(i).wait_send()
        for stage in range(stages):
            step(i, stage).wait_send()


def combine(n_fs, sums):
    owners, tokens, features = sums.shape
    n_bits = n_fs.bit_length() - 1
    stages, rows = n_bits + 1, tokens // 2
    chunks = plan_of(n_bits, features)
    dma = pltpu.SemaphoreType.DMA
    vmem = pl.BlockSpec(memory_space=pltpu.VMEM)
    boxes = [
        pltpu.VMEM((*(2,) * (n_bits - stage), rows, size), BF16)
        for _, _, size in chunks for stage in range(stages)
    ]
    view = (*(2,) * (n_bits + 1), rows, features)
    return pl.pallas_call(
        functools.partial(combine_kernel, n_fs, chunks),
        out_shape=jax.ShapeDtypeStruct((tokens, features), BF16),
        in_specs=[vmem],
        out_specs=vmem,
        scratch_shapes=[
            pltpu.VMEM(view, BF16),
            *boxes,
            dma((len(chunks), stages)),
            dma((len(chunks), stages)),
            dma((len(chunks),)),
            dma((len(chunks),)),
        ],
        compiler_params=pltpu.CompilerParams(
            collective_id=1, has_side_effects=True, vmem_limit_bytes=40 * 1024 * 1024
        ),
    )(sums.reshape(view))


def plain_local(tokens, route_ids, route_logits, norm_gain, gate_master, up_master, down_master):
    gain_rows = norm_gain[None, :, None]
    gate_half = (gate_master * gain_rows).astype(jnp.bfloat16)
    up_half = (up_master * gain_rows).astype(jnp.bfloat16)
    down_half = down_master.astype(jnp.bfloat16)
    gate_cols, up_cols, down_cols = (
        lax.all_to_all(gate_half, "tp", split_axis=0, concat_axis=2, tiled=True),
        lax.all_to_all(up_half, "tp", split_axis=0, concat_axis=2, tiled=True),
        lax.all_to_all(down_half, "tp", split_axis=0, concat_axis=2, tiled=True),
    )
    gate_part, up_part = (
        lax.all_to_all(gate_cols, "fs", split_axis=2, concat_axis=1, tiled=True),
        lax.all_to_all(up_cols, "fs", split_axis=2, concat_axis=1, tiled=True),
    )
    gate_weight, up_weight, down_weight = (
        lax.all_gather(gate_part, "gr", axis=1, tiled=True),
        lax.all_gather(up_part, "gr", axis=1, tiled=True),
        lax.all_gather(down_cols, "gr", axis=2, tiled=True),
    )
    as_float = tokens.astype(jnp.float32)
    normed = (
        as_float * lax.rsqrt(jnp.mean(as_float * as_float, axis=-1, keepdims=True) + epsilon)
    ).astype(jnp.bfloat16)
    differ = route_logits[:, 0] - route_logits[:, 1]
    route_weight = jnp.stack([jax.nn.sigmoid(differ), jax.nn.sigmoid(-differ)], axis=1)
    experts_here = gate_weight.shape[0]
    first_expert = lax.axis_index("tp") * experts_here
    expert_ids = first_expert + jnp.arange(experts_here, dtype=jnp.int32)
    route_hits = route_ids[None, :, :] == expert_ids[:, None, None]
    chosen = jnp.any(route_hits, axis=2)
    weight_rows = jnp.sum(jnp.where(route_hits, route_weight[None, :, :], 0.0), axis=2)
    slot_rank = jnp.cumsum(chosen.astype(jnp.int32), axis=1) - 1
    slot_ids = jnp.arange(CAP, dtype=jnp.int32)
    picker = chosen[:, None, :] & (slot_rank[:, None, :] == slot_ids[None, :, None])
    picker_float = picker.astype(jnp.float32)
    packed = jnp.einsum(
        "xsr,rd->sxd", picker.astype(jnp.bfloat16), normed, preferred_element_type=jnp.float32
    ).astype(jnp.bfloat16)
    slot_weight = jnp.einsum(
        "xsr,xr->sx", picker_float, weight_rows, precision=lax.Precision.HIGHEST
    )
    pieces = lax.all_gather(packed, "fs", axis=0, tiled=True)
    gate_act = jnp.einsum("kxd,xdh->kxh", pieces, gate_weight, preferred_element_type=jnp.float32)
    up_act = jnp.einsum("kxd,xdh->kxh", pieces, up_weight, preferred_element_type=jnp.float32)
    hidden = (jax.nn.silu(gate_act) * up_act).astype(jnp.bfloat16)
    expert_out = lax.psum_scatter(
        jnp.einsum("kxh,xhd->kxd", hidden, down_weight, preferred_element_type=jnp.float32).astype(
            jnp.bfloat16
        ),
        "fs",
        scatter_dimension=0,
        tiled=True,
    ).astype(jnp.float32)
    weighted = expert_out * slot_weight[:, :, None]
    block_sum = jnp.einsum("xsr,sxd->rd", picker_float, weighted, precision=lax.Precision.HIGHEST)
    mixed = lax.psum(block_sum.astype(jnp.bfloat16), "tp")
    return (gate_weight, up_weight, down_weight, mixed)


def fast_local(sizes, tokens, route_ids, route_logits, norm_gain, gate_master, up_master, down_master):
    n_gr, n_fs, n_tp = sizes
    as_float = tokens.astype(jnp.float32)
    normed = (
        as_float * lax.rsqrt(jnp.mean(as_float * as_float, axis=-1, keepdims=True) + epsilon)
    ).astype(jnp.bfloat16)
    differ = route_logits[:, 0] - route_logits[:, 1]
    route_weight = jnp.stack([jax.nn.sigmoid(differ), jax.nn.sigmoid(-differ)], axis=1)
    experts_here = gate_master.shape[0] // n_tp
    first_expert = lax.axis_index("tp") * experts_here
    expert_ids = first_expert + jnp.arange(experts_here, dtype=jnp.int32)
    route_hits = route_ids[None, :, :] == expert_ids[:, None, None]
    chosen = jnp.any(route_hits, axis=2)
    weight_rows = jnp.sum(jnp.where(route_hits, route_weight[None, :, :], 0.0), axis=2)
    slot_rank = jnp.cumsum(chosen.astype(jnp.int32), axis=1) - 1
    slot_ids = jnp.arange(CAP, dtype=jnp.int32)
    picker = chosen[:, None, :] & (slot_rank[:, None, :] == slot_ids[None, :, None])
    combiner = (picker.astype(jnp.float32) * weight_rows[:, None, :]).astype(jnp.bfloat16)
    share = tokens.shape[1] // n_tp
    strip = lax.dynamic_slice_in_dim(normed, lax.axis_index("tp") * share, share, axis=1)
    gate_moved, up_moved, down_moved, blocks = exchange(
        sizes, norm_gain, gate_master, up_master, down_master,
        jnp.concatenate([strip, combiner.reshape(-1, tokens.shape[0])], axis=1),
    )
    gate_weight, up_weight, down_weight, sums = run_experts(
        blocks, gate_moved, up_moved, down_moved
    )
    return (gate_weight, up_weight, down_weight, combine(n_fs, sums))


def solution(mesh):
    n_gr, n_fs, n_tp = (mesh.shape[name] for name in ("gr", "fs", "tp"))
    placed = (
        P(("gr", "fs"), None),
        P(("gr", "fs"), None),
        P(("gr", "fs"), None),
        P(("gr", "fs")),
        P(None, ("gr", "fs"), "tp"),
        P(None, ("gr", "fs"), "tp"),
        P(None, "fs", ("gr", "tp")),
    )

    def local(tokens, route_ids, route_logits, norm_gain, gate_master, up_master, down_master):
        width = gate_master.shape[2] * n_tp // n_fs
        aligned = width % 128 == 0 and down_master.shape[2] % 128 == 0
        fits = n_fs % n_tp == 0 and n_fs & (n_fs - 1) == 0 and n_fs > 2
        fits = fits and n_gr > 1 and n_tp == 2 and tokens.shape[0] % 128 == 0
        fits = fits and gate_master.shape[0] // n_tp * CAP == tokens.shape[0]
        run = functools.partial(fast_local, (n_gr, n_fs, n_tp)) if aligned and fits else plain_local
        return run(tokens, route_ids, route_logits, norm_gain, gate_master, up_master, down_master)

    return jax.shard_map(
        local,
        mesh=mesh,
        in_specs=placed,
        out_specs=(
            P("tp", None, "fs"),
            P("tp", None, "fs"),
            P("tp", "fs", None),
            P(("gr", "fs"), None),
        ),
        check_vma=False,
    )
```

```python
import functools

import jax
import jax.numpy as jnp
from jax import lax
from jax.experimental import pallas as pl
from jax.experimental.pallas import tpu as pltpu
from jax.sharding import PartitionSpec as P

CAP = 32


epsilon = 1e-06
MESH = pl.DeviceIdType.MESH
BF16 = jnp.bfloat16


def prepare_kernel(per_plane, tokens_ref, ids_ref, logits_ref, gain_ref, piece, gain_out):
    rows, share = tokens_ref.shape[0], piece.shape[1] - tokens_ref.shape[0]
    tp = lax.axis_index("tp")
    values = tokens_ref[...].astype(jnp.float32)
    scale = lax.rsqrt(jnp.mean(values * values, axis=-1, keepdims=True) + epsilon)
    half = tokens_ref[:, pl.ds(pl.multiple_of(tp * share, share), share)]
    piece[:, pl.ds(0, share)] = (half.astype(jnp.float32) * scale).astype(BF16)

    down = lax.broadcasted_iota(jnp.int32, (rows, rows), 0)
    right = lax.broadcasted_iota(jnp.int32, (rows, rows), 1)

    def column(line):
        return jnp.sum(jnp.where(down == right, line, 0.0), axis=1, keepdims=True)

    gain_out[...] = column(gain_ref[...])
    ids = ids_ref[...].astype(jnp.float32)
    differ = column(logits_ref[0:1, :] - logits_ref[1:2, :])
    expert = (right // CAP + tp * per_plane).astype(jnp.float32)
    first, second = column(ids[0:1, :]) == expert, column(ids[1:2, :]) == expert
    weight = jnp.where(first, jax.nn.sigmoid(differ), 0.0)
    weight = weight + jnp.where(second, jax.nn.sigmoid(-differ), 0.0)
    hits = jnp.where(first | second, 1.0, 0.0)
    upto = jnp.where(right <= down, 1.0, 0.0).astype(BF16)
    rank = jnp.dot(upto, hits.astype(BF16), preferred_element_type=jnp.float32)
    slot = (right % CAP + 1).astype(jnp.float32)
    kept = jnp.where(rank == slot, hits * weight, 0.0)
    piece[:, pl.ds(share, rows)] = kept.astype(BF16)


def prepare(n_tp, experts, tokens, route_ids, route_logits, norm_gain):
    rows, features = tokens.shape
    return pl.pallas_call(
        functools.partial(prepare_kernel, experts),
        out_shape=(
            pltpu.VMEM((rows, features // n_tp + rows), BF16),
            pltpu.VMEM((norm_gain.shape[0], 1), jnp.float32),
        ),
        name="prepare",
    )(tokens, route_ids.T, route_logits.T, norm_gain[None, :])


def exchange_kernel(
    n_gr, n_fs, n_tp,
    gain_ref, gate_ref, up_ref, down_ref, packed_ref,
    gate_out, up_out, down_out, pieces,
    stage, stage_down, crossed, raw, raw_down,
    load_sem, load_down_sem, x_send, x_recv, s_send, s_recv, own_sem,
    d_send, d_recv, xd_send, xd_recv, own_down_sem, dd_send, dd_recv,
    p_send, p_recv, p_own, q_send, q_recv,
):
    gr, fs, tp = (lax.axis_index(name) for name in ("gr", "fs", "tp"))
    experts, _, width = gate_out.shape
    rows, cols = gate_ref.shape[1], gate_ref.shape[2]
    per = cols // width
    down_cols = down_ref.shape[2]
    masters, outs = (gate_ref, up_ref), (gate_out, up_out)

    barrier = pltpu.get_barrier_semaphore()
    peers = 0
    for o in range(1, n_tp):
        pl.semaphore_signal(barrier, 1, device_id=(gr, fs, lax.rem(tp + o, n_tp)), device_id_type=MESH)
        peers += 1
    for k in range(1, n_fs):
        pl.semaphore_signal(barrier, 1, device_id=(gr, lax.rem(fs + k, n_fs), tp), device_id_type=MESH)
        peers += 1
    for o in range(1, n_gr):
        pl.semaphore_signal(barrier, 1, device_id=(lax.rem(gr + o, n_gr), fs, tp), device_id_type=MESH)
        peers += 1

    def tp_at(o):
        return lax.rem(tp + o, n_tp)

    order = [(w, o) for w in range(2) for o in [*range(1, n_tp), 0]]

    def load(e, w, o):
        return pltpu.make_async_copy(
            masters[w].at[tp_at(o) * experts + e], raw.at[w, o], load_sem.at[w, o]
        )

    def load_down(e, o):
        return pltpu.make_async_copy(
            down_ref.at[tp_at(o) * experts + e], raw_down.at[o], load_down_sem.at[o]
        )

    def over_tp(e, w, o, j):
        columns = pl.ds(j * width, width)
        return pltpu.make_async_remote_copy(
            stage.at[w, o, e, :, columns], crossed.at[w, o - 1, e, :, columns],
            x_send.at[w, o - 1, e, j], x_recv.at[w, o - 1, e, j],
            device_id=(gr, fs, tp_at(o)), device_id_type=MESH,
        )

    def rows_of(group, owner):
        return pl.ds(pl.multiple_of((group * n_fs + owner) * rows, rows), rows)

    def source(e, w, o, j):
        columns = pl.ds(j * width, width)
        if o == 0:
            return stage.at[w, 0, e, :, columns]
        return crossed.at[w, o - 1, e, :, columns]

    def fan(e, w, o):
        begin = lax.rem(tp - o + n_tp, n_tp) * per
        for j in range(per):
            if o:
                over_tp(e, w, o, j).wait_recv()
            to = begin + j
            k = lax.rem(to - fs + n_fs, n_fs)
            target = outs[w].at[e, rows_of(gr, fs)]

            @pl.when(to != fs)
            def _():
                pltpu.make_async_remote_copy(
                    source(e, w, o, j), target, s_send.at[w, e, k], s_recv.at[w, e, k],
                    device_id=(gr, to, tp), device_id_type=MESH,
                ).start()

            @pl.when(to == fs)
            def _():
                pltpu.make_async_copy(source(e, w, o, j), target, own_sem.at[w, e]).start()

    def arrival(e, w, k):
        piece = outs[w].at[e, rows_of(gr, lax.rem(fs - k + n_fs, n_fs))]
        return pltpu.make_async_remote_copy(
            piece, piece, s_send.at[w, e, k], s_recv.at[w, e, k],
            device_id=(gr, lax.rem(fs + k, n_fs), tp), device_id_type=MESH,
        )

    def own_copy(e, w):
        return pltpu.make_async_copy(
            source(e, w, 0, 0), outs[w].at[e, rows_of(gr, fs)], own_sem.at[w, e]
        )

    def over_gr(e, w, k, o, group):
        piece = outs[w].at[e, rows_of(group, lax.rem(fs - k + n_fs, n_fs))]
        return pltpu.make_async_remote_copy(
            piece, piece, d_send.at[w, e, k, o - 1], d_recv.at[w, e, k, o - 1],
            device_id=(lax.rem(gr + o, n_gr), fs, tp), device_id_type=MESH,
        )

    def down_block(group, t):
        return pl.ds(pl.multiple_of((group * n_tp + t) * down_cols, down_cols), down_cols)

    def down_over_tp(e, o):
        return pltpu.make_async_remote_copy(
            stage_down.at[o, e], down_out.at[e, :, down_block(gr, tp)],
            xd_send.at[o - 1, e], xd_recv.at[o - 1, e],
            device_id=(gr, fs, tp_at(o)), device_id_type=MESH,
        )

    def down_arrival(e, o):
        piece = down_out.at[e, :, down_block(gr, lax.rem(tp - o + n_tp, n_tp))]
        return pltpu.make_async_remote_copy(
            piece, piece, xd_send.at[o - 1, e], xd_recv.at[o - 1, e],
            device_id=(gr, fs, tp_at(o)), device_id_type=MESH,
        )

    def down_own(e):
        return pltpu.make_async_copy(
            stage_down.at[0, e], down_out.at[e, :, down_block(gr, tp)], own_down_sem.at[e]
        )

    def down_over_gr(e, s, o, group):
        piece = down_out.at[e, :, down_block(group, lax.rem(tp - s + n_tp, n_tp))]
        return pltpu.make_async_remote_copy(
            piece, piece, dd_send.at[e, s, o - 1], dd_recv.at[e, s, o - 1],
            device_id=(lax.rem(gr + o, n_gr), fs, tp), device_id_type=MESH,
        )

    pairs = n_fs // 2
    z, y = fs // 2, lax.rem(fs, 2)

    depth = packed_ref.shape[0] // experts
    share = packed_ref.shape[1] - packed_ref.shape[0]

    def strip(e):
        return pl.ds(e * depth, depth)

    def relay(kind, hop, e):
        at = {"up": z - hop, "down": z + hop, "over": z - hop, "over_down": z + hop}[kind]
        to = {"up": fs + 2, "down": fs - 2}.get(kind, fs + 1 - 2 * y)
        origin = at * 2 + y
        here = packed_ref.at[strip(e)] if hop == 0 else pieces.at[tp, origin, strip(e)]
        slot = ["up", "down", "over", "over_down"].index(kind)
        return pltpu.make_async_remote_copy(
            here, pieces.at[tp, origin, strip(e)], p_send.at[slot, hop, e], p_recv.at[origin, e],
            device_id=(gr, to, tp), device_id_type=MESH,
        )

    def landed(origin, e):
        piece = pieces.at[tp, origin, strip(e)]
        return pltpu.make_async_remote_copy(
            piece, piece, p_send.at[0, 0, e], p_recv.at[origin, e],
            device_id=(gr, fs + 1 - 2 * y, tp), device_id_type=MESH,
        )

    def relayed(kind, hop):
        if kind == "up":
            return (z - hop >= 0) & (z + 1 < pairs)
        if kind == "down":
            return (z + hop < pairs) & (z >= 1)
        return z - hop >= 0 if kind == "over" else z + hop < pairs

    def relay_start(kind, hop, e):
        @pl.when(relayed(kind, hop))
        def _():
            relay(kind, hop, e).start()

    def relay_from(hop):
        for e in range(experts):
            @pl.when(z - hop >= 0)
            def _():
                landed((z - hop) * 2 + y, e).wait_recv()

            relay_start("up", hop, e)
            relay_start("over", hop, e)

            @pl.when(z + hop < pairs)
            def _():
                landed((z + hop) * 2 + y, e).wait_recv()

            relay_start("down", hop, e)
            relay_start("over_down", hop, e)

    own_piece = pltpu.make_async_copy(packed_ref, pieces.at[tp, fs], p_own)

    def across(origin, side):
        part = pieces.at[side, origin, :, pl.ds(0, share)]
        return pltpu.make_async_remote_copy(
            part, part, q_send.at[origin], q_recv.at[origin],
            device_id=(gr, fs, tp_at(1)), device_id_type=MESH,
        )

    for w, o in order:
        load(0, w, o).start()
    for o in range(n_tp):
        load_down(0, o).start()
    pl.semaphore_wait(barrier, peers)
    for kind in ("up", "down", "over"):
        for e in range(experts):
            relay_start(kind, 0, e)
    own_piece.start()

    def cast(e, leg):
        for w, o in order:
            if (o > 0) != (leg == "tp"):
                continue
            load(e, w, o).wait()
            stage[w, o, e] = (raw[w, o] * gain_ref[...]).astype(BF16)

            @pl.when(e + 1 < experts)
            def _():
                load(e + 1, w, o).start()

            if o:
                for j in range(per):
                    over_tp(e, w, o, j).start()
            else:
                fan(e, w, 0)

    def forward(e):
        for w in range(2):
            for o in range(1, n_tp):
                fan(e, w, o)

    cast(0, "tp")
    for hop in range(1, pairs):
        relay_from(hop)
    cast(0, "fs")

    @pl.loop(1, experts)
    def _(e):
        cast(e, "tp")
        cast(e, "fs")
        forward(e - 1)

    own_piece.wait()
    for at in range(pairs):
        for e in range(experts):
            landed(at * 2 + 1 - y, e).wait_recv()

    @pl.loop(0, n_fs)
    def _(origin):
        across(origin, tp).start()

    @pl.loop(0, experts)
    def _(e):
        for o in [*range(1, n_tp), 0]:
            load_down(e, o).wait()
            stage_down[o, e] = raw_down[o].astype(BF16)

            @pl.when(e + 1 < experts)
            def _():
                load_down(e + 1, o).start()

            if o:
                down_over_tp(e, o).start()
            else:
                down_own(e).start()

    def collect(e):
        for w in range(2):
            own_copy(e, w).wait()
            for o in range(1, n_gr):
                over_gr(e, w, 0, o, gr).start()

        @pl.loop(1, n_fs)
        def _(k):
            for w in range(2):
                arrival(e, w, k).wait_recv()
                for o in range(1, n_gr):
                    over_gr(e, w, k, o, gr).start()

    forward(experts - 1)

    @pl.loop(0, experts - 1)
    def _(e):
        collect(e)

    @pl.loop(0, experts)
    def _(e):
        down_own(e).wait()
        for s in range(1, n_tp):
            down_arrival(e, s).wait_recv()
        for s in range(n_tp):
            for o in range(1, n_gr):
                down_over_gr(e, s, o, gr).start()

    collect(experts - 1)

    @pl.loop(0, experts)
    def _(e):
        for w in range(2):
            for o in range(1, n_tp):
                for j in range(per):
                    over_tp(e, w, o, j).wait_send()

            @pl.loop(1, n_fs)
            def _(k):
                arrival(e, w, k).wait_send()

            @pl.loop(0, n_fs)
            def _(k):
                for o in range(1, n_gr):
                    over_gr(e, w, k, o, gr).wait_send()
                    over_gr(e, w, k, o, lax.rem(gr - o + n_gr, n_gr)).wait_recv()

        for s in range(1, n_tp):
            down_over_tp(e, s).wait_send()
        for s in range(n_tp):
            for o in range(1, n_gr):
                down_over_gr(e, s, o, gr).wait_send()
                down_over_gr(e, s, o, lax.rem(gr - o + n_gr, n_gr)).wait_recv()

    @pl.loop(0, n_fs)
    def _(origin):
        across(origin, tp).wait_send()
        across(origin, 1 - tp).wait_recv()

    for kind in ("up", "down", "over", "over_down"):
        for hop in range(1 if kind == "over_down" else 0, pairs):
            @pl.when(relayed(kind, hop))
            def _():
                for e in range(experts):
                    relay(kind, hop, e).wait_send()


def exchange(sizes, gain, gate_master, up_master, down_master, packed):
    n_gr, n_fs, n_tp = sizes
    all_experts, rows, cols = gate_master.shape
    experts = all_experts // n_tp
    width = cols * n_tp // n_fs
    hidden, down_cols = down_master.shape[1], down_master.shape[2]
    any_spec = pl.BlockSpec(memory_space=pl.ANY)
    dma = pltpu.SemaphoreType.DMA
    up_shape = jax.ShapeDtypeStruct((experts, rows * n_gr * n_fs, width), BF16)
    return pl.pallas_call(
        functools.partial(exchange_kernel, n_gr, n_fs, n_tp),
        out_shape=(
            up_shape,
            up_shape,
            jax.ShapeDtypeStruct((experts, hidden, down_cols * n_gr * n_tp), BF16),
            jax.ShapeDtypeStruct((n_tp, n_fs, *packed.shape), BF16),
        ),
        in_specs=[pl.BlockSpec(memory_space=pltpu.VMEM), *[any_spec] * 4],
        out_specs=(any_spec,) * 4,
        scratch_shapes=[
            pltpu.VMEM((2, n_tp, experts, rows, cols), BF16),
            pltpu.VMEM((n_tp, experts, hidden, down_cols), BF16),
            pltpu.VMEM((2, n_tp - 1, experts, rows, cols), BF16),
            pltpu.VMEM((2, n_tp, rows, cols), jnp.float32),
            pltpu.VMEM((n_tp, hidden, down_cols), jnp.float32),
            dma((2, n_tp)),
            dma((n_tp,)),
            dma((2, n_tp - 1, experts, n_fs // n_tp)),
            dma((2, n_tp - 1, experts, n_fs // n_tp)),
            dma((2, experts, n_fs)),
            dma((2, experts, n_fs)),
            dma((2, experts)),
            dma((2, experts, n_fs, n_gr - 1)),
            dma((2, experts, n_fs, n_gr - 1)),
            dma((n_tp - 1, experts)),
            dma((n_tp - 1, experts)),
            dma((experts,)),
            dma((experts, n_tp, n_gr - 1)),
            dma((experts, n_tp, n_gr - 1)),
            dma((4, n_fs // 2, experts)),
            dma((n_fs, experts)),
            dma,
            dma((n_fs,)),
            dma((n_fs,)),
        ],
        compiler_params=pltpu.CompilerParams(
            collective_id=0, has_side_effects=True, vmem_limit_bytes=52 * 1024 * 1024
        ),
        cost_estimate=pl.CostEstimate(flops=0, bytes_accessed=1_000_000_000, transcendentals=0),
    )(gain, gate_master, up_master, down_master, packed)


def experts_kernel(
    slices, lead,
    blocks, gate_in, up_in, down_in,
    gate_out, up_out, down_out, sums,
    tall, wide, pieces, partial, gate_act, up_act, hidden,
    tall_load, tall_store, wide_load, wide_store,
):
    experts, features, width = gate_in.shape
    depth, cols = tall.shape[1], wide.shape[2]
    steps, ring = 2 * slices, tall.shape[0]
    count = hidden.shape[1]
    owners, tokens = sums.shape[0], sums.shape[1]
    ins, outs = (gate_in, up_in), (gate_out, up_out)

    def tall_ends(refs, e, j):
        return refs[j % 2].at[e, pl.ds(j // 2 * depth, depth)]

    def tall_slot(e, j):
        return lax.rem(e * steps + j, ring)

    def load_tall(e, j):
        slot = tall_slot(e, j)
        return pltpu.make_async_copy(tall_ends(ins, e, j), tall.at[slot], tall_load.at[slot])

    def store_tall(e, j):
        slot = tall_slot(e, j)
        return pltpu.make_async_copy(tall.at[slot], tall_ends(outs, e, j), tall_store.at[slot])

    def span(c):
        return pl.ds(pl.multiple_of(c * cols, cols), cols)

    def load_wide(c, e):
        slot = c * experts + e
        return pltpu.make_async_copy(down_in.at[e, :, span(c)], wide.at[slot], wide_load.at[slot])

    def store_wide(c, e):
        slot = c * experts + e
        return pltpu.make_async_copy(wide.at[slot], down_out.at[e, :, span(c)], wide_store.at[slot])

    for j in range(lead):
        load_tall(j // steps, j % steps).start()

    tp = lax.axis_index("tp")
    share = blocks.shape[3] - tokens

    @pl.loop(0, owners)
    def _(o):
        picker = (blocks[tp, o, :, pl.ds(share, tokens)].astype(jnp.float32) > 0).astype(BF16)
        for side in range(blocks.shape[0]):
            rows = lax.dot_general(
                picker, blocks[side, o, :, pl.ds(0, share)], (((0,), (0,)), ((), ())),
                preferred_element_type=jnp.float32,
            ).astype(BF16)
            pieces[:, o, :, pl.ds(side * share, share)] = rows.reshape(experts, -1, share)

    @pl.loop(0, experts)
    def _(e):
        for j in range(steps):
            load_tall(e, j).wait()
            store_tall(e, j).start()
            later, k = e + (j + lead) // steps, (j + lead) % steps

            @pl.when(later < experts)
            def _():
                @pl.when(later * steps + k >= ring)
                def _():
                    before = later * steps + k - ring
                    store_tall(before // steps, k).wait()

                load_tall(later, k).start()

            @pl.when(e == experts - 1)
            def _():
                for i in range(j, slices * experts // 2, steps):
                    load_wide(i // experts, i % experts).start()

            act = (gate_act, up_act)[j % 2]
            x = pieces[e, :, :, pl.ds(j // 2 * depth, depth)].reshape(count, depth)
            value = jnp.dot(x, tall[tall_slot(e, j)], preferred_element_type=jnp.float32)
            if j < 2:
                act[...] = value
            else:
                act[...] += value
        hidden[e] = (jax.nn.silu(gate_act[...]) * up_act[...]).astype(BF16)

    half = slices * experts // 2

    @pl.loop(0, slices)
    def _(c):
        for e in range(experts):
            load_wide(c, e).wait()
            store_wide(c, e).start()
            ahead = c * experts + e + half

            @pl.when(ahead < slices * experts)
            def _():
                load_wide(ahead // experts, lax.rem(ahead, experts)).start()

            value = jnp.dot(hidden[e], wide[c * experts + e], preferred_element_type=jnp.float32)
            partial[e] = value.astype(BF16).reshape(partial.shape[1:])

        for o in range(owners):
            weights = blocks[tp, o, :, pl.ds(share, tokens)]
            rows = partial[:, o].reshape(-1, cols)
            sums[o, :, span(c)] = jnp.dot(
                weights, rows, preferred_element_type=jnp.float32
            ).astype(BF16)

    for i in range(ring):
        at = experts * steps - ring + i
        store_tall(at // steps, at % steps).wait()
    for c in range(slices):
        for e in range(experts):
            store_wide(c, e).wait()


def run_experts(blocks, gate, up, down):
    experts, features, width = gate.shape
    _, owners, tokens, _ = blocks.shape
    cap, slices = tokens // experts, 4
    count = owners * cap
    ring = 2 * 2 * slices
    any_spec = pl.BlockSpec(memory_space=pl.ANY)
    vmem = pl.BlockSpec(memory_space=pltpu.VMEM)
    dma = pltpu.SemaphoreType.DMA
    return pl.pallas_call(
        functools.partial(experts_kernel, slices, 3 * slices),
        out_shape=(
            jax.ShapeDtypeStruct(gate.shape, BF16),
            jax.ShapeDtypeStruct(up.shape, BF16),
            jax.ShapeDtypeStruct(down.shape, BF16),
            pltpu.VMEM((owners, tokens, features), BF16),
        ),
        in_specs=[vmem, any_spec, any_spec, any_spec],
        out_specs=(any_spec, any_spec, any_spec, vmem),
        scratch_shapes=[
            pltpu.VMEM((ring, features // slices, width), BF16),
            pltpu.VMEM((slices * experts, width, features // slices), BF16),
            pltpu.VMEM((experts, owners, cap, features), BF16),
            pltpu.VMEM((experts, owners, cap, features // slices), BF16),
            pltpu.VMEM((count, width), jnp.float32),
            pltpu.VMEM((count, width), jnp.float32),
            pltpu.VMEM((experts, count, width), BF16),
            dma((ring,)),
            dma((ring,)),
            dma((slices * experts,)),
            dma((slices * experts,)),
        ],
        compiler_params=pltpu.CompilerParams(vmem_limit_bytes=50 * 1024 * 1024),
        cost_estimate=pl.CostEstimate(
            flops=6 * experts * count * features * width,
            bytes_accessed=12 * experts * features * width, transcendentals=0,
        ),
    )(blocks, gate, up, down)


def plan_of(n_bits, features):
    rest = list(range(2, n_bits))
    orders = ([0, "x", 1, *rest], ["x", 1, 0, *rest], [1, 0, "x", *rest])
    unit = 128
    units = features // unit
    shares, chunks, begin = [], [], 0
    for i in range(6):
        shares.append(-((sum(shares) - units) // (6 - i)))
    for i, share in enumerate(shares):
        if share:
            chunks.append((orders[i % 3], begin * unit, share * unit))
        begin += share
    return chunks


def combine_kernel(n_fs, chunks, sums, out, acc, *rest):
    stages = len(chunks[0][0])
    boxes, (s_send, s_recv, o_send, o_recv) = rest[:-4], rest[-4:]
    gr, fs, tp = (lax.axis_index(name) for name in ("gr", "fs", "tp"))
    n_bits = stages - 1
    rows = sums.shape[-2]
    bits = [lax.rem(fs // (1 << b), 2) for b in range(n_bits)]

    def mine(dim):
        return tp if dim == "x" else bits[dim]

    def partner(dim):
        if dim == "x":
            return (gr, fs, 1 - tp)
        return (gr, fs + (1 - 2 * bits[dim]) * (1 << dim), tp)

    def block(order, stage, own, cols):
        index = [slice(None)] * (n_bits + 1)
        for dim in order[: stage + 1]:
            at = n_bits if dim == "x" else n_bits - 1 - dim
            index[at] = mine(dim)
            if dim == order[stage] and not own:
                index[at] = 1 - mine(dim)
        return (*index, slice(None), cols)

    barrier = pltpu.get_barrier_semaphore()
    for dim in [*range(n_bits), "x"]:
        pl.semaphore_signal(barrier, 1, device_id=partner(dim), device_id_type=MESH)
    pl.semaphore_wait(barrier, n_bits + 1)

    def step(i, stage):
        order, begin, size = chunks[i]
        held = sums if stage == 0 else acc
        return pltpu.make_async_remote_copy(
            held.at[block(order, stage, False, pl.ds(begin, size))],
            boxes[i * stages + stage], s_send.at[i, stage], s_recv.at[i, stage],
            device_id=partner(order[stage]), device_id_type=MESH,
        )

    def finished(i):
        _, begin, size = chunks[i]
        here = out.at[pl.ds(pl.multiple_of(tp * rows, rows), rows), pl.ds(begin, size)]
        return pltpu.make_async_remote_copy(
            here, here, o_send.at[i], o_recv.at[i], device_id=partner("x"), device_id_type=MESH
        )

    for i in range(len(chunks)):
        step(i, 0).start()
    for stage in range(stages):
        for i, (order, begin, size) in enumerate(chunks):
            step(i, stage).wait_recv()
            at = block(order, stage, True, pl.ds(begin, size))
            held = sums if stage == 0 else acc
            value = held[at].astype(jnp.float32) + boxes[i * stages + stage][...].astype(jnp.float32)
            if stage + 1 < stages:
                acc[at] = value.astype(BF16)
                step(i, stage + 1).start()
            else:
                out[pl.ds(pl.multiple_of(tp * rows, rows), rows), pl.ds(begin, size)] = value.astype(BF16)
                finished(i).start()
    for i in range(len(chunks)):
        _, begin, size = chunks[i]
        there = out.at[pl.ds(pl.multiple_of((1 - tp) * rows, rows), rows), pl.ds(begin, size)]
        pltpu.make_async_remote_copy(
            there, there, o_send.at[i], o_recv.at[i], device_id=partner("x"), device_id_type=MESH
        ).wait_recv()
        finished(i).wait_send()
        for stage in range(stages):
            step(i, stage).wait_send()


def combine(n_fs, sums):
    owners, tokens, features = sums.shape
    n_bits = n_fs.bit_length() - 1
    stages, rows = n_bits + 1, tokens // 2
    chunks = plan_of(n_bits, features)
    dma = pltpu.SemaphoreType.DMA
    vmem = pl.BlockSpec(memory_space=pltpu.VMEM)
    boxes = [
        pltpu.VMEM((*(2,) * (n_bits - stage), rows, size), BF16)
        for _, _, size in chunks for stage in range(stages)
    ]
    view = (*(2,) * (n_bits + 1), rows, features)
    return pl.pallas_call(
        functools.partial(combine_kernel, n_fs, chunks),
        out_shape=jax.ShapeDtypeStruct((tokens, features), BF16),
        in_specs=[vmem],
        out_specs=vmem,
        scratch_shapes=[
            pltpu.VMEM(view, BF16),
            *boxes,
            dma((len(chunks), stages)),
            dma((len(chunks), stages)),
            dma((len(chunks),)),
            dma((len(chunks),)),
        ],
        compiler_params=pltpu.CompilerParams(
            collective_id=1, has_side_effects=True, vmem_limit_bytes=40 * 1024 * 1024
        ),
    )(sums.reshape(view))


def plain_local(tokens, route_ids, route_logits, norm_gain, gate_master, up_master, down_master):
    gain_rows = norm_gain[None, :, None]
    gate_half = (gate_master * gain_rows).astype(jnp.bfloat16)
    up_half = (up_master * gain_rows).astype(jnp.bfloat16)
    down_half = down_master.astype(jnp.bfloat16)
    gate_cols, up_cols, down_cols = (
        lax.all_to_all(gate_half, "tp", split_axis=0, concat_axis=2, tiled=True),
        lax.all_to_all(up_half, "tp", split_axis=0, concat_axis=2, tiled=True),
        lax.all_to_all(down_half, "tp", split_axis=0, concat_axis=2, tiled=True),
    )
    gate_part, up_part = (
        lax.all_to_all(gate_cols, "fs", split_axis=2, concat_axis=1, tiled=True),
        lax.all_to_all(up_cols, "fs", split_axis=2, concat_axis=1, tiled=True),
    )
    gate_weight, up_weight, down_weight = (
        lax.all_gather(gate_part, "gr", axis=1, tiled=True),
        lax.all_gather(up_part, "gr", axis=1, tiled=True),
        lax.all_gather(down_cols, "gr", axis=2, tiled=True),
    )
    as_float = tokens.astype(jnp.float32)
    normed = (
        as_float * lax.rsqrt(jnp.mean(as_float * as_float, axis=-1, keepdims=True) + epsilon)
    ).astype(jnp.bfloat16)
    differ = route_logits[:, 0] - route_logits[:, 1]
    route_weight = jnp.stack([jax.nn.sigmoid(differ), jax.nn.sigmoid(-differ)], axis=1)
    experts_here = gate_weight.shape[0]
    first_expert = lax.axis_index("tp") * experts_here
    expert_ids = first_expert + jnp.arange(experts_here, dtype=jnp.int32)
    route_hits = route_ids[None, :, :] == expert_ids[:, None, None]
    chosen = jnp.any(route_hits, axis=2)
    weight_rows = jnp.sum(jnp.where(route_hits, route_weight[None, :, :], 0.0), axis=2)
    slot_rank = jnp.cumsum(chosen.astype(jnp.int32), axis=1) - 1
    slot_ids = jnp.arange(CAP, dtype=jnp.int32)
    picker = chosen[:, None, :] & (slot_rank[:, None, :] == slot_ids[None, :, None])
    picker_float = picker.astype(jnp.float32)
    packed = jnp.einsum(
        "xsr,rd->sxd", picker.astype(jnp.bfloat16), normed, preferred_element_type=jnp.float32
    ).astype(jnp.bfloat16)
    slot_weight = jnp.einsum(
        "xsr,xr->sx", picker_float, weight_rows, precision=lax.Precision.HIGHEST
    )
    pieces = lax.all_gather(packed, "fs", axis=0, tiled=True)
    gate_act = jnp.einsum("kxd,xdh->kxh", pieces, gate_weight, preferred_element_type=jnp.float32)
    up_act = jnp.einsum("kxd,xdh->kxh", pieces, up_weight, preferred_element_type=jnp.float32)
    hidden = (jax.nn.silu(gate_act) * up_act).astype(jnp.bfloat16)
    expert_out = lax.psum_scatter(
        jnp.einsum("kxh,xhd->kxd", hidden, down_weight, preferred_element_type=jnp.float32).astype(
            jnp.bfloat16
        ),
        "fs",
        scatter_dimension=0,
        tiled=True,
    ).astype(jnp.float32)
    weighted = expert_out * slot_weight[:, :, None]
    block_sum = jnp.einsum("xsr,sxd->rd", picker_float, weighted, precision=lax.Precision.HIGHEST)
    mixed = lax.psum(block_sum.astype(jnp.bfloat16), "tp")
    return (gate_weight, up_weight, down_weight, mixed)


def fast_local(sizes, tokens, route_ids, route_logits, norm_gain, gate_master, up_master, down_master):
    n_gr, n_fs, n_tp = sizes
    packed, gain = prepare(
        n_tp, gate_master.shape[0] // n_tp, tokens, route_ids, route_logits, norm_gain
    )
    gate_moved, up_moved, down_moved, blocks = exchange(
        sizes, gain, gate_master, up_master, down_master, packed
    )
    gate_weight, up_weight, down_weight, sums = run_experts(
        blocks, gate_moved, up_moved, down_moved
    )
    return (gate_weight, up_weight, down_weight, combine(n_fs, sums))


def solution(mesh):
    n_gr, n_fs, n_tp = (mesh.shape[name] for name in ("gr", "fs", "tp"))
    placed = (
        P(("gr", "fs"), None),
        P(("gr", "fs"), None),
        P(("gr", "fs"), None),
        P(("gr", "fs")),
        P(None, ("gr", "fs"), "tp"),
        P(None, ("gr", "fs"), "tp"),
        P(None, "fs", ("gr", "tp")),
    )

    def local(tokens, route_ids, route_logits, norm_gain, gate_master, up_master, down_master):
        width = gate_master.shape[2] * n_tp // n_fs
        aligned = width % 128 == 0 and down_master.shape[2] % 128 == 0
        fits = n_fs % n_tp == 0 and n_fs & (n_fs - 1) == 0 and n_fs > 2
        fits = fits and n_gr > 1 and n_tp == 2 and tokens.shape[0] % 128 == 0
        fits = fits and gate_master.shape[0] // n_tp * CAP == tokens.shape[0]
        fits = fits and norm_gain.shape[0] == tokens.shape[0]
        run = functools.partial(fast_local, (n_gr, n_fs, n_tp)) if aligned and fits else plain_local
        return run(tokens, route_ids, route_logits, norm_gain, gate_master, up_master, down_master)

    return jax.shard_map(
        local,
        mesh=mesh,
        in_specs=placed,
        out_specs=(
            P("tp", None, "fs"),
            P("tp", None, "fs"),
            P("tp", "fs", None),
            P(("gr", "fs"), None),
        ),
        check_vma=False,
    )
```
